32 devices in a mesh: kv: 8 (over z, y), tp: 4 (over x, core).
Axes of the slice: x: 2, y: 2, z: 4, core: 2. Of those that a mesh axis runs over, the one named last changes fastest.
Arguments:
- tokens: bfloat16 [8, 2048], P(None, 'kv'), may hold values from -6 to 6
- in_gain: float32 [2048], P('kv'), may hold values from 0.1 to 1.9
- w_query: bfloat16 [2048, 512], P('kv', 'tp'), may hold values from -0.125 to 0.125
- score_bias: float32 [4], P('tp'), as said below
- cache_keys: bfloat16 [8, 8192, 512], P(None, 'kv', 'tp'), may hold values from -8 to 8, as said below
- cache_values: bfloat16 [8, 8192, 512], P(None, 'kv', 'tp'), may hold values from -6 to 6
- lengths: int32 [8], replicated, may hold values from 1024 to 8192, as said below
- head_gain: float32 [512], P('tp'), may hold values from 0.1 to 1.9
- w_out: bfloat16 [512, 2048], P('tp', 'kv'), may hold values from -0.25 to 0.25
Outputs:
- mixed: bfloat16 [8, 2048], P(None, 'kv')
The draws below stay inside these ranges and needn't reach their ends.
Inputs may be any that keep to these rules, and one draw needn't show every extreme that they name: `score_bias`: one value a head, added to every score of that head. `cache_keys`: real-valued key entries. `lengths`: one sequence has all 8192 positions cached.
All inputs are finite; a program needn't handle non-finite values.
Results may differ from the reference program's by a relative error of at most 0.0095.
The reference program's roundings to bfloat16 on the way (of `gained`, `queries`, `weights` and `normed`) count: a program that leaves them out, or rounds other values in their place, can miss the bound.
Values may be sent and summed in bfloat16 or wider, within the bound.
No kernel may reach another device: no remote copies, remote signals or barrier semaphores. Data moves between devices by JAX's collectives and lax.ppermute only.
A program may use at most 64 MiB of HBM per device.

```python
import jax
import jax.numpy as jnp
from jax import lax

D = 2048
HEADS = 4
DH = 128
SEQS = 8
POS_DEV = 1024
SEQ_LEN = 8192
N_TP = 4


def draw_score_bias(key, part):
    key_order, key_slow, key_fast = jax.random.split(jax.random.fold_in(key, 11), 3)
    slow_heads = jax.random.permutation(key_order, HEADS) < HEADS // 2
    slow_value = -jnp.log(jnp.float32(SEQ_LEN)) + jax.random.uniform(key_slow, (HEADS,), jnp.float32, -0.6, 0.0)
    fast_value = -jnp.log(jax.random.uniform(key_fast, (HEADS,), jnp.float32, 30.0, 100.0)) - 1.1
    return jnp.where(slow_heads, slow_value, fast_value).astype(jnp.float32)


def draw_cache_keys(key, part):
    key_scale, key_base = jax.random.split(jax.random.fold_in(key, 3))
    spans = SEQ_LEN // 32
    span_scale = jax.random.uniform(key_scale, (SEQS, spans, 1, HEADS, 1), jnp.float32, 0.5, 2.0)
    unit_draw = jnp.clip(jax.random.normal(key_base, (SEQS, spans, 32, HEADS, DH), jnp.float32), -4.0, 4.0)
    return (unit_draw * span_scale).reshape(SEQS, SEQ_LEN, HEADS * DH).astype(jnp.bfloat16)


def draw_lengths(key, part):
    key_lens, key_full = jax.random.split(jax.random.fold_in(key, 7))
    drawn = jax.random.randint(key_lens, (SEQS,), SEQ_LEN // 8, SEQ_LEN + 1)
    chosen = jax.random.randint(key_full, (), 0, SEQS)
    return jnp.where(jnp.arange(SEQS) == chosen, SEQ_LEN, drawn).astype(jnp.int32)


def level_of(rng, dims, cuts, least, largest):
    level, own = 1.0, jax.random.fold_in(rng, 6)
    for dim, parts in cuts:
        heights = jnp.exp(jax.random.uniform(jax.random.fold_in(own, dim), (parts,), jnp.float32, least / len(cuts), largest / len(cuts)))
        level = level * jnp.repeat(heights, dims[dim] // parts).reshape([-1 if axis == dim else 1 for axis in range(len(dims))])
    return level


def bell_draw(stream_key, extent, deviation, reach, shards=(), kind=jnp.bfloat16):
    values = deviation * jax.random.normal(stream_key, extent, jnp.float32)
    if shards:
        values = values * level_of(stream_key, extent, shards, -0.22, 0.18)
    return jnp.clip(values, -reach, reach).astype(kind)


def setup_inputs(seed: int = 0) -> dict:
    key_of = jax.random.split(jax.random.key(seed), 10)
    tokens = bell_draw(key_of[0], (SEQS, D), 1.0, 6.0, ((1, 8),))
    in_gain = jnp.clip(1.0 + 0.18 * jax.random.normal(key_of[1], (D,), jnp.float32), 0.1, 1.9)
    w_query = bell_draw(key_of[2], (D, HEADS * DH), D ** -0.5, 0.125, ((0, 8), (1, 4)))
    score_bias = draw_score_bias(jax.random.fold_in(key_of[9], 71), 0)
    cache_keys = draw_cache_keys(jax.random.fold_in(key_of[9], 71), 0)
    cache_values = bell_draw(key_of[5], (SEQS, SEQ_LEN, HEADS * DH), 1.0, 6.0, ((1, 8), (2, 4)))
    lengths = draw_lengths(jax.random.fold_in(key_of[9], 71), 0)
    head_gain = jnp.clip(1.0 + 0.18 * jax.random.normal(key_of[7], (HEADS * DH,), jnp.float32), 0.1, 1.9)
    w_out = bell_draw(key_of[8], (HEADS * DH, D), (HEADS * DH) ** -0.5, 0.25, ((0, 4), (1, 8)))
    return dict(tokens=tokens, in_gain=in_gain, w_query=w_query, score_bias=score_bias, cache_keys=cache_keys, cache_values=cache_values, lengths=lengths, head_gain=head_gain, w_out=w_out)


EPS = 1e-06

def reference(tokens, in_gain, w_query, score_bias, cache_keys, cache_values, lengths, head_gain, w_out):
    as_float = tokens.astype(jnp.float32)
    gained = (as_float * in_gain).astype(jnp.bfloat16)
    raw_query = jnp.dot(gained, w_query, preferred_element_type=jnp.float32)
    row_scale = lax.rsqrt(lax.optimization_barrier(jnp.mean(as_float * as_float, axis=1)) + EPS)
    queries = (raw_query * row_scale[:, None]).astype(jnp.bfloat16).reshape(SEQS, HEADS, DH)
    segments = SEQ_LEN // POS_DEV

    def per_sequence(fields):
        seq_query, seq_keys, seq_values, seq_len = fields
        keys_f32 = seq_keys.astype(jnp.float32).reshape(SEQ_LEN, HEADS, DH)
        scores = jnp.einsum('hd,lhd->hl', seq_query.astype(jnp.float32), keys_f32) * DH ** (-0.5)
        scores = scores + score_bias[:, None]
        usable = (jnp.arange(SEQ_LEN, dtype=jnp.int32) < seq_len)[None, :]
        log_keep = jnp.where(usable, jax.nn.log_sigmoid(-scores), 0.0)
        segmented = log_keep.reshape(HEADS, segments, POS_DEV)
        suffix = lax.cumsum(segmented, axis=2, reverse=True) - segmented
        gate_log = jax.nn.log_sigmoid(scores).reshape(HEADS, segments, POS_DEV)
        weights = jnp.where(usable.reshape(1, segments, POS_DEV), jnp.exp(gate_log + suffix), 0.0)
        weights = weights.astype(jnp.bfloat16)
        values_f32 = seq_values.astype(jnp.float32).reshape(segments, POS_DEV, HEADS, DH)
        seg_out = jnp.einsum('hnp,nphd->hnd', weights.astype(jnp.float32), values_f32)
        totals = lax.optimization_barrier(jnp.sum(segmented, axis=2))
        later_sum = lax.cumsum(totals, axis=1, reverse=True) - totals
        return lax.optimization_barrier(jnp.sum(seg_out * jnp.exp(later_sum)[..., None], axis=1))
    attended = lax.map(per_sequence, (queries, cache_keys, cache_values, lengths))
    mean_sq = lax.optimization_barrier(jnp.mean(attended * attended, axis=2))
    normed = attended * lax.rsqrt(mean_sq + EPS)[..., None]
    normed = (normed.reshape(SEQS, HEADS * DH) * head_gain).astype(jnp.bfloat16)
    block_width = HEADS * DH // N_TP
    mixed = jnp.zeros((SEQS, D), jnp.float32)
    for block in range(N_TP):
        part_out = jnp.dot(normed[:, block * block_width:(block + 1) * block_width], w_out[block * block_width:(block + 1) * block_width], preferred_element_type=jnp.float32)
        mixed = mixed + lax.optimization_barrier(part_out.astype(jnp.bfloat16)).astype(jnp.float32)
    return mixed.astype(jnp.bfloat16)
```

```python
import jax
import jax.numpy as jnp
from jax import lax
from jax.sharding import PartitionSpec as P

EPS = 1e-06


def exchange(value, axis):
    size = lax.axis_size(axis)
    copies = jnp.broadcast_to(value[None], (size,) + value.shape)
    return lax.all_to_all(copies, axis, 0, 0, tiled=False)


def shards(
    tokens, in_gain, w_query, score_bias, cache_keys, cache_values, lengths, head_gain, w_out
):
    sequences = tokens.shape[0]
    local_len = cache_keys.shape[1]
    head_width = cache_keys.shape[2]
    heads_here = score_bias.shape[0]
    head_size = head_width // heads_here
    kv_size = lax.axis_size("kv")
    tp_size = lax.axis_size("tp")
    width = tokens.shape[1] * kv_size
    as_float = tokens.astype(jnp.float32)
    gained = (as_float * in_gain).astype(jnp.bfloat16)
    partial_value = jnp.dot(gained, w_query, preferred_element_type=jnp.float32)
    squares = jnp.sum(as_float * as_float, axis=1, keepdims=True)
    packed = jnp.concatenate([partial_value, jnp.broadcast_to(squares, (sequences, 128))], axis=1)
    gathered = jnp.sum(exchange(packed, "kv"), axis=0)
    summed = gathered[:, :head_width]
    total_sq = gathered[:, head_width : head_width + 1]
    row_scale = lax.rsqrt(total_sq / width + EPS)
    queries = (summed * row_scale).astype(jnp.bfloat16).reshape(sequences, heads_here, head_size)
    key_heads = cache_keys.reshape(sequences, local_len, heads_here, head_size)
    value_heads = cache_values.reshape(sequences, local_len, heads_here, head_size)
    scores = jnp.einsum("bhd,bphd->bhp", queries, key_heads, preferred_element_type=jnp.float32)
    scores = scores * head_size ** (-0.5) + score_bias[None, :, None]
    here = lax.axis_index("kv")
    places = here * local_len + lax.iota(jnp.int32, local_len)
    usable = places[None, None, :] < lengths[:, None, None]
    log_keep = jnp.where(usable, jax.nn.log_sigmoid(-scores), 0.0)
    strict_upper = (
        lax.iota(jnp.int32, local_len)[:, None] > lax.iota(jnp.int32, local_len)[None, :]
    ).astype(jnp.float32)
    suffix = jnp.einsum("bhr,rs->bhs", log_keep, strict_upper, precision=lax.Precision.HIGHEST)
    weights = jnp.where(usable, jnp.exp(jax.nn.log_sigmoid(scores) + suffix), 0.0).astype(
        jnp.bfloat16
    )
    local_out = jnp.einsum(
        "bhp,bphd->bhd", weights, value_heads, preferred_element_type=jnp.float32
    )
    seg_total = jnp.sum(log_keep, axis=2, keepdims=True)
    packed = jnp.concatenate(
        [local_out, jnp.broadcast_to(seg_total, (sequences, heads_here, 128))], axis=2
    )
    every = exchange(packed, "kv")
    every_out = every[..., :head_size]
    totals = every[..., head_size : head_size + 1]
    later_sum = lax.cumsum(totals, axis=0, reverse=True) - totals
    attended = jnp.sum(every_out * jnp.exp(later_sum), axis=0)
    mean_sq = jnp.mean(attended * attended, axis=2)
    normed = attended * lax.rsqrt(mean_sq + EPS)[..., None]
    normed = (normed.reshape(sequences, head_width) * head_gain).astype(jnp.bfloat16)
    part_out = jnp.dot(normed, w_out, preferred_element_type=jnp.float32).astype(jnp.bfloat16)
    mixed = part_out.astype(jnp.float32)
    for shift in range(tp_size - 1, 0, -1):
        moved = lax.ppermute(part_out, "tp", [(i, i ^ shift) for i in range(tp_size)])
        mixed = mixed + moved.astype(jnp.float32)
    return mixed.astype(jnp.bfloat16)


def solution(mesh):
    return jax.shard_map(
        shards,
        mesh=mesh,
        in_specs=(
            P(None, "kv"),
            P("kv"),
            P("kv", "tp"),
            P("tp"),
            P(None, "kv", "tp"),
            P(None, "kv", "tp"),
            P(),
            P("tp"),
            P("tp", "kv"),
        ),
        out_specs=P(None, "kv"),
        check_vma=False,
    )
```

```python
import functools

import jax
import jax.numpy as jnp
from jax import lax
from jax.experimental import pallas as pl
from jax.experimental.pallas import tpu as pltpu
from jax.sharding import PartitionSpec as P

EPS = 1e-06
LANES = 128
VMEM = pl.BlockSpec(memory_space=pltpu.VMEM)
SMEM = pl.BlockSpec(memory_space=pltpu.SMEM)
F32 = jnp.float32
BF16 = jnp.bfloat16


def three_terms(value):
    high = value.astype(BF16)
    rest = value - high.astype(F32)
    middle = rest.astype(BF16)
    low = (rest - middle.astype(F32)).astype(BF16)
    return high, middle, low


def query_kernel(tokens_ref, gain_ref, w_ref, head_gain_ref, w_out_ref, packed_ref, block_ref):
    as_float = tokens_ref[...].astype(F32)
    gained = (as_float * gain_ref[...]).astype(BF16)
    partial_value = jnp.dot(gained, w_ref[...], preferred_element_type=F32)
    squares = jnp.sum(as_float * as_float, axis=1, keepdims=True)
    squares = jnp.broadcast_to(squares, (as_float.shape[0], LANES))
    packed = jnp.concatenate([partial_value, squares], axis=1)
    for device in range(packed_ref.shape[0]):
        packed_ref[device] = packed
    rows, columns = w_out_ref.shape
    if columns < block_ref.shape[1]:
        block_ref[...] = jnp.zeros_like(block_ref)
    block_ref[:rows, :columns] = w_out_ref[...]
    high, middle, low = three_terms(head_gain_ref[...])
    row = lax.broadcasted_iota(jnp.int32, (16, rows), 0)
    gains = jnp.where(row == 0, high.astype(F32), 0.0)
    gains = jnp.where(row == 1, middle.astype(F32), gains)
    gains = jnp.where(row == 2, low.astype(F32), gains)
    block_ref[rows : rows + 16, :rows] = gains.astype(BF16)


def attention_kernel(
    width, gathered_ref, bias_ref, lengths_ref, here_ref, keys_ref, values_ref, packed_ref
):
    sequences, local_len, head_size = keys_ref.shape
    tiles = local_len // LANES
    gathered = jnp.sum(gathered_ref[...], axis=0)
    row_scale = lax.rsqrt(gathered[:, head_size:] / width + EPS)
    queries = gathered[:, :head_size] * row_scale
    row = lax.broadcasted_iota(jnp.int32, (sequences, head_size), 0)
    spread = jnp.concatenate(
        [jnp.where(row == b, queries, 0.0) for b in range(sequences)], axis=1
    ).astype(BF16)
    keys = jnp.concatenate([keys_ref[b] for b in range(sequences)], axis=1)
    scores = lax.dot_general(
        spread, keys, (((1,), (1,)), ((), ())), preferred_element_type=F32
    )
    scores = scores * head_size ** (-0.5) + bias_ref[0]
    place = lax.broadcasted_iota(jnp.int32, (sequences, local_len), 1)
    place = place + here_ref[0] * local_len
    sequence = lax.broadcasted_iota(jnp.int32, (sequences, local_len), 0)
    limit = jnp.zeros((sequences, local_len), jnp.int32)
    for b in range(sequences):
        limit = jnp.where(sequence == b, lengths_ref[b], limit)
    usable = place < limit
    soft = jnp.log1p(jnp.exp(-jnp.abs(scores)))
    log_keep = jnp.where(usable, -jnp.maximum(scores, 0.0) - soft, 0.0)
    log_gate = jnp.minimum(scores, 0.0) - soft
    stacked = jnp.concatenate(
        [log_keep[:, t * LANES : (t + 1) * LANES] for t in range(tiles)], axis=0
    )
    terms = jnp.concatenate(three_terms(stacked), axis=0)
    r = lax.broadcasted_iota(jnp.int32, (LANES, 2 * LANES), 0)
    s = lax.broadcasted_iota(jnp.int32, (LANES, 2 * LANES), 1)
    later = jnp.where((r > s) | (s >= LANES), 1.0, 0.0).astype(BF16)
    sums = jnp.dot(terms, later, preferred_element_type=F32)
    count = tiles * sequences
    sums = sums[:count] + sums[count : 2 * count] + sums[2 * count :]
    running = jnp.zeros((sequences, LANES), F32)
    suffixes = [None] * tiles
    for t in reversed(range(tiles)):
        block = sums[t * sequences : (t + 1) * sequences]
        suffixes[t] = block[:, :LANES] + running
        running = running + block[:, LANES:]
    suffix = jnp.concatenate(suffixes, axis=1)
    weights = jnp.where(usable, jnp.exp(log_gate + suffix), 0.0).astype(BF16)
    values = jnp.concatenate([values_ref[b] for b in range(sequences)], axis=1)
    products = jnp.dot(weights, values, preferred_element_type=F32)
    out = jnp.zeros((sequences, head_size), F32)
    for b in range(sequences):
        out = jnp.where(row == b, products[:, b * head_size : (b + 1) * head_size], out)
    high, middle, low = three_terms(running)
    lane = lax.broadcasted_iota(jnp.int32, (sequences, LANES), 1)
    total = jnp.where(lane == 0, high.astype(F32), 0.0)
    total = jnp.where(lane == 1, middle.astype(F32), total)
    total = jnp.where(lane == 2, low.astype(F32), total)
    packed = jnp.concatenate([out, total], axis=0).astype(BF16)
    for device in range(packed_ref.shape[0]):
        packed_ref[device] = packed


def output_kernel(kv_size, order, me_ref, every_ref, *refs):
    blocks, mixed_ref, normed_ref = refs[:-2], refs[-2], refs[-1]
    heads = len(blocks)
    sequences = mixed_ref.shape[0]
    columns = mixed_ref.shape[1]
    head_size = every_ref.shape[2]
    place = {}
    for index, device in enumerate(order):
        place[device] = index
    totals = jnp.concatenate(
        [every_ref[d, sequences:, :] for d in range(kv_size * heads)], axis=0
    )
    ones = jnp.ones((LANES, LANES), BF16)
    totals = jnp.dot(totals, ones, preferred_element_type=F32)
    for head in range(heads):
        later_sum = jnp.zeros((sequences, head_size), F32)
        attended = jnp.zeros((sequences, head_size), F32)
        for n in reversed(range(kv_size)):
            d = place[n * heads + head]
            out = every_ref[d, :sequences, :].astype(F32)
            attended = attended + out * jnp.exp(later_sum)
            later_sum = later_sum + totals[d * sequences : (d + 1) * sequences]
        mean_sq = jnp.mean(attended * attended, axis=1, keepdims=True)
        normed_ref[head] = attended * lax.rsqrt(mean_sq + EPS)
    parts = []
    for shift in range(heads):
        block = blocks[shift]
        gain = jnp.sum(block[head_size : head_size + 16, :head_size].astype(F32), axis=0, keepdims=True)
        normed = (normed_ref[me_ref[0] ^ shift] * gain).astype(BF16)
        part = jnp.dot(normed, block[:head_size, :columns], preferred_element_type=F32)
        parts.append(part.astype(BF16).astype(F32))
    while len(parts) > 1:
        parts = [parts[i] + parts[i + 1] for i in range(0, len(parts), 2)]
    mixed_ref[...] = parts[0].astype(BF16)


def led_by(leader, size):
    return [leader] + [i for i in range(size) if i != leader]


def shards(
    tokens, in_gain, w_query, score_bias, cache_keys, cache_values, lengths, head_gain, w_out
):
    sequences, features = tokens.shape
    head_width = cache_keys.shape[2]
    assert score_bias.shape[0] == 1 and head_width == LANES
    kv_size = lax.axis_size("kv")
    tp_size = lax.axis_size("tp")
    devices = kv_size * tp_size
    columns = w_out.shape[1]
    packed, block = pl.pallas_call(
        query_kernel,
        out_shape=(
            jax.ShapeDtypeStruct((kv_size, sequences, 2 * LANES), F32),
            jax.ShapeDtypeStruct((head_width + 16, max(columns, LANES)), BF16),
        ),
        in_specs=[VMEM] * 5,
        out_specs=(VMEM, VMEM),
    )(tokens, in_gain[None], w_query, head_gain[None], w_out)
    first = led_by(kv_size // 4, kv_size)
    gathered = lax.all_to_all(packed, "kv", 0, 0, axis_index_groups=[first], tiled=False)
    blocks = [block]
    for shift in range(1, tp_size):
        blocks.append(lax.ppermute(block, "tp", [(i, i ^ shift) for i in range(tp_size)]))
    here = lax.axis_index("kv").astype(jnp.int32)[None]
    me = lax.axis_index("tp").astype(jnp.int32)[None]
    packed = pl.pallas_call(
        functools.partial(attention_kernel, features * kv_size),
        out_shape=jax.ShapeDtypeStruct((devices, 2 * sequences, LANES), BF16),
        in_specs=[VMEM, SMEM, SMEM, SMEM, VMEM, VMEM],
        out_specs=VMEM,
    )(gathered, score_bias, lengths, here, cache_keys, cache_values)
    order = led_by((kv_size // 2 - 1) * tp_size + 1, devices)
    every = lax.all_to_all(
        packed, ("kv", "tp"), 0, 0, axis_index_groups=[order], tiled=False
    )
    return pl.pallas_call(
        functools.partial(output_kernel, kv_size, order),
        out_shape=jax.ShapeDtypeStruct((sequences, columns), BF16),
        in_specs=[SMEM] + [VMEM] * (1 + tp_size),
        out_specs=VMEM,
        scratch_shapes=[pltpu.VMEM((tp_size, sequences, LANES), F32)],
    )(me, every, *blocks)


def solution(mesh):
    return jax.shard_map(
        shards,
        mesh=mesh,
        in_specs=(
            P(None, "kv"),
            P("kv"),
            P("kv", "tp"),
            P("tp"),
            P(None, "kv", "tp"),
            P(None, "kv", "tp"),
            P(),
            P("tp"),
            P("tp", "kv"),
        ),
        out_specs=P(None, "kv"),
        check_vma=False,
    )
```

```python
import functools

import jax
import jax.numpy as jnp
from jax import lax
from jax.experimental import pallas as pl
from jax.experimental.pallas import tpu as pltpu
from jax.sharding import PartitionSpec as P

EPS = 1e-06
LANES = 128
VMEM = pl.BlockSpec(memory_space=pltpu.VMEM)
SMEM = pl.BlockSpec(memory_space=pltpu.SMEM)
HBM = pl.BlockSpec(memory_space=pltpu.HBM)
F32 = jnp.float32
BF16 = jnp.bfloat16


def three_terms(value):
    high = value.astype(BF16)
    rest = value - high.astype(F32)
    middle = rest.astype(BF16)
    low = (rest - middle.astype(F32)).astype(BF16)
    return high, middle, low


def query_kernel(
    tokens_hbm, in_gain_hbm, w_hbm, bias_hbm, lengths_hbm, head_gain_hbm,
    packed_ref, side_ref,
    tokens_ref, in_gain_ref, w_ref, bias_ref, lengths_ref, head_gain_ref, sems,
):
    pairs = (
        (w_hbm, w_ref),
        (tokens_hbm, tokens_ref),
        (in_gain_hbm, in_gain_ref),
        (lengths_hbm, lengths_ref),
        (bias_hbm, bias_ref),
        (head_gain_hbm, head_gain_ref),
    )
    copies = [
        pltpu.make_async_copy(src, dst, sems.at[i]) for i, (src, dst) in enumerate(pairs)
    ]
    for copy in copies:
        copy.start()
    for copy in copies[1:]:
        copy.wait()
    as_float = tokens_ref[...].astype(F32)
    sequences = as_float.shape[0]
    gained = (as_float * in_gain_ref[...]).astype(BF16)
    squares = jnp.sum(as_float * as_float, axis=1, keepdims=True)
    squares = jnp.broadcast_to(squares, (sequences, LANES))
    row = lax.broadcasted_iota(jnp.int32, (2 * sequences, LANES), 0)
    side = jnp.where(row == sequences, bias_ref[0, 0], 0.0)
    side = jnp.where(row == sequences + 1, head_gain_ref[...], side)
    for b in range(sequences):
        side = jnp.where(row == b, lengths_ref[0, b].astype(F32), side)
    side_ref[...] = side
    copies[0].wait()
    partial_value = jnp.dot(gained, w_ref[...], preferred_element_type=F32)
    packed = jnp.concatenate([partial_value, squares], axis=1)
    for device in range(packed_ref.shape[0]):
        packed_ref[device] = packed


def attention_kernel(width, gathered_ref, side_ref, keys_ref, values_ref, packed_ref):
    sequences, local_len, head_size = keys_ref.shape
    tiles = local_len // LANES
    gathered = jnp.sum(gathered_ref[...], axis=0)
    row_scale = lax.rsqrt(gathered[:, head_size:] / width + EPS)
    queries = gathered[:, :head_size] * row_scale
    row = lax.broadcasted_iota(jnp.int32, (sequences, head_size), 0)
    lane = lax.broadcasted_iota(jnp.int32, (sequences, LANES), 1)
    spread = jnp.concatenate(
        [jnp.where(row == b, queries, 0.0) for b in range(sequences)], axis=1
    ).astype(BF16)
    keys = jnp.concatenate([keys_ref[b] for b in range(sequences)], axis=1)
    scores = lax.dot_general(
        spread, keys, (((1,), (1,)), ((), ())), preferred_element_type=F32
    )
    bias = side_ref[sequences : sequences + 1, :]
    bias = jnp.concatenate([bias] * tiles, axis=1)
    scores = scores * head_size ** (-0.5) + bias
    here = lax.axis_index("kv") * local_len
    limit = side_ref[:sequences, :].astype(jnp.int32) - here
    usable = jnp.concatenate([lane + t * LANES < limit for t in range(tiles)], axis=1)
    soft = jnp.log1p(jnp.exp(-jnp.abs(scores)))
    log_keep = jnp.where(usable, -jnp.maximum(scores, 0.0) - soft, 0.0)
    log_gate = jnp.minimum(scores, 0.0) - soft
    stacked = jnp.concatenate(
        [log_keep[:, t * LANES : (t + 1) * LANES] for t in range(tiles)], axis=0
    )
    terms = jnp.concatenate(three_terms(stacked), axis=0)
    r = lax.broadcasted_iota(jnp.int32, (LANES, 2 * LANES), 0)
    s = lax.broadcasted_iota(jnp.int32, (LANES, 2 * LANES), 1)
    later = jnp.where((r > s) | (s >= LANES), 1.0, 0.0).astype(BF16)
    sums = jnp.dot(terms, later, preferred_element_type=F32)
    count = tiles * sequences
    sums = sums[:count] + sums[count : 2 * count] + sums[2 * count :]
    running = jnp.zeros((sequences, LANES), F32)
    suffixes = [None] * tiles
    for t in reversed(range(tiles)):
        block = sums[t * sequences : (t + 1) * sequences]
        suffixes[t] = block[:, :LANES] + running
        running = running + block[:, LANES:]
    suffix = jnp.concatenate(suffixes, axis=1)
    weights = jnp.where(usable, jnp.exp(log_gate + suffix), 0.0).astype(BF16)
    values = jnp.concatenate([values_ref[b] for b in range(sequences)], axis=1)
    products = jnp.dot(weights, values, preferred_element_type=F32)
    out = jnp.zeros((sequences, head_size), F32)
    for b in range(sequences):
        out = jnp.where(row == b, products[:, b * head_size : (b + 1) * head_size], out)
    packed = jnp.concatenate([out, running], axis=1)
    for device in range(packed_ref.shape[0]):
        packed_ref[device] = packed


def output_kernel(order, every_ref, side_ref, w_out_ref, part_ref):
    size, sequences, _ = every_ref.shape
    place = {device: index for index, device in enumerate(order)}
    later_sum = jnp.zeros((sequences, LANES), F32)
    attended = jnp.zeros((sequences, LANES), F32)
    for n in reversed(range(size)):
        d = place[n]
        attended = attended + every_ref[d, :, :LANES] * jnp.exp(later_sum)
        later_sum = later_sum + every_ref[d, :, LANES:]
    mean_sq = jnp.mean(attended * attended, axis=1, keepdims=True)
    gain = side_ref[sequences + 1 : sequences + 2, :]
    normed = (attended * lax.rsqrt(mean_sq + EPS) * gain).astype(BF16)
    part = jnp.dot(normed, w_out_ref[...], preferred_element_type=F32)
    part_ref[...] = part.astype(BF16)


def mix_kernel(*refs):
    parts = [ref[...].astype(F32) for ref in refs[:-1]]
    while len(parts) > 1:
        parts = [parts[i] + parts[i + 1] for i in range(0, len(parts), 2)]
    refs[-1][...] = parts[0].astype(BF16)


def led_by(leader, size):
    return [leader] + [i for i in range(size) if i != leader]


def shards(
    tokens, in_gain, w_query, score_bias, cache_keys, cache_values, lengths, head_gain, w_out
):
    sequences, features = tokens.shape
    head_width = cache_keys.shape[2]
    assert score_bias.shape[0] == 1 and head_width == LANES
    kv_size = lax.axis_size("kv")
    tp_size = lax.axis_size("tp")
    columns = w_out.shape[1]
    packed, side = pl.pallas_call(
        query_kernel,
        out_shape=(
            jax.ShapeDtypeStruct((kv_size, sequences, 2 * LANES), F32),
            jax.ShapeDtypeStruct((2 * sequences, LANES), F32),
        ),
        in_specs=[HBM] * 6,
        out_specs=(VMEM, VMEM),
        scratch_shapes=[
            pltpu.VMEM(tokens.shape, BF16),
            pltpu.VMEM((1, features), F32),
            pltpu.VMEM(w_query.shape, BF16),
            pltpu.SMEM((1, 1), F32),
            pltpu.SMEM((1, sequences), jnp.int32),
            pltpu.VMEM((1, head_width), F32),
            pltpu.SemaphoreType.DMA((6,)),
        ],
        compiler_params=pltpu.CompilerParams(vmem_limit_bytes=4 << 20),
        cost_estimate=pl.CostEstimate(flops=1 << 33, bytes_accessed=128 << 20, transcendentals=0),
    )(*[
        x if x.size == 1 else pltpu.with_memory_space_constraint(x, pltpu.HBM)
        for x in (tokens, in_gain[None], w_query, score_bias[None], lengths[None], head_gain[None])
    ])
    first = led_by(kv_size * 5 // 8, kv_size)
    gathered = lax.all_to_all(packed, "kv", 0, 0, axis_index_groups=[first], tiled=False)
    packed = pl.pallas_call(
        functools.partial(attention_kernel, features * kv_size),
        out_shape=jax.ShapeDtypeStruct((kv_size, sequences, 2 * LANES), F32),
        in_specs=[VMEM, VMEM, VMEM, VMEM],
        out_specs=VMEM,
        compiler_params=pltpu.CompilerParams(vmem_limit_bytes=24 << 20),
    )(gathered, side, cache_keys, cache_values)
    second = led_by(kv_size * 5 // 8, kv_size)
    every = lax.all_to_all(packed, "kv", 0, 0, axis_index_groups=[second], tiled=False)
    part = pl.pallas_call(
        functools.partial(output_kernel, second),
        out_shape=jax.ShapeDtypeStruct((sequences, columns), BF16),
        in_specs=[VMEM] * 3,
        out_specs=VMEM,
        compiler_params=pltpu.CompilerParams(vmem_limit_bytes=4 << 20),
    )(every, side, w_out)
    parts = {0: part}
    for shift in range(tp_size - 1, 0, -1):
        parts[shift] = lax.ppermute(part, "tp", [(i, i ^ shift) for i in range(tp_size)])
    return pl.pallas_call(
        mix_kernel,
        out_shape=jax.ShapeDtypeStruct((sequences, columns), BF16),
        in_specs=[VMEM] * tp_size,
        out_specs=VMEM,
        compiler_params=pltpu.CompilerParams(vmem_limit_bytes=4 << 20),
    )(*[parts[shift] for shift in range(tp_size)])


def solution(mesh):
    return jax.shard_map(
        shards,
        mesh=mesh,
        in_specs=(
            P(None, "kv"),
            P("kv"),
            P("kv", "tp"),
            P("tp"),
            P(None, "kv", "tp"),
            P(None, "kv", "tp"),
            P(),
            P("tp"),
            P("tp", "kv"),
        ),
        out_specs=P(None, "kv"),
        check_vma=False,
    )
```

```python
import functools

import jax
import jax.numpy as jnp
from jax import lax
from jax.experimental import pallas as pl
from jax.experimental.pallas import tpu as pltpu
from jax.sharding import PartitionSpec as P

EPS = 1e-06
LANES = 128
VMEM = pl.BlockSpec(memory_space=pltpu.VMEM)
SMEM = pl.BlockSpec(memory_space=pltpu.SMEM)
HBM = pl.BlockSpec(memory_space=pltpu.HBM)
F32 = jnp.float32
BF16 = jnp.bfloat16


def three_terms(value):
    high = value.astype(BF16)
    rest = value - high.astype(F32)
    middle = rest.astype(BF16)
    low = (rest - middle.astype(F32)).astype(BF16)
    return high, middle, low


def opening_kernel(seed_ref):
    seed_ref[...] = jnp.zeros_like(seed_ref)


def query_kernel(
    seed_ref, tokens_ref, in_gain_ref, w_ref, bias_ref, lengths_ref, head_gain_ref,
    packed_ref, side_ref,
):
    as_float = tokens_ref[...].astype(F32)
    sequences = as_float.shape[0]
    gained = (as_float * in_gain_ref[...]).astype(BF16)
    squares = jnp.sum(as_float * as_float, axis=1, keepdims=True)
    squares = jnp.broadcast_to(squares, (sequences, LANES))
    row = lax.broadcasted_iota(jnp.int32, (2 * sequences, LANES), 0)
    side = jnp.where(row == sequences, bias_ref[...], 0.0)
    side = jnp.where(row == sequences + 1, head_gain_ref[...], side)
    lengths = lengths_ref[...].astype(F32)
    own = lax.broadcasted_iota(jnp.int32, (2 * sequences, sequences), 0)
    own = own == lax.broadcasted_iota(jnp.int32, (2 * sequences, sequences), 1)
    lengths = jnp.sum(jnp.where(own, lengths, 0.0), axis=1, keepdims=True)
    side = jnp.where(row < sequences, lengths, side)
    side_ref[...] = side + seed_ref[:1]
    partial_value = jnp.dot(gained, w_ref[...], preferred_element_type=F32)
    packed = jnp.concatenate([partial_value, squares], axis=1)
    for device in range(packed_ref.shape[0]):
        packed_ref[device] = packed


def attention_kernel(width, gathered_ref, side_ref, keys_ref, values_ref, packed_ref):
    sequences, local_len, head_size = keys_ref.shape
    tiles = local_len // LANES
    gathered = jnp.sum(gathered_ref[...], axis=0)
    row_scale = lax.rsqrt(gathered[:, head_size:] / width + EPS)
    queries = gathered[:, :head_size] * row_scale
    row = lax.broadcasted_iota(jnp.int32, (sequences, head_size), 0)
    lane = lax.broadcasted_iota(jnp.int32, (sequences, LANES), 1)
    spread = jnp.concatenate(
        [jnp.where(row == b, queries, 0.0) for b in range(sequences)], axis=1
    ).astype(BF16)
    keys = jnp.concatenate([keys_ref[b] for b in range(sequences)], axis=1)
    scores = lax.dot_general(
        spread, keys, (((1,), (1,)), ((), ())), preferred_element_type=F32
    )
    bias = side_ref[sequences : sequences + 1, :]
    bias = jnp.concatenate([bias] * tiles, axis=1)
    scores = scores * head_size ** (-0.5) + bias
    here = lax.axis_index("kv") * local_len
    limit = side_ref[:sequences, :].astype(jnp.int32) - here
    usable = jnp.concatenate([lane + t * LANES < limit for t in range(tiles)], axis=1)
    soft = jnp.log1p(jnp.exp(-jnp.abs(scores)))
    log_keep = jnp.where(usable, -jnp.maximum(scores, 0.0) - soft, 0.0)
    log_gate = jnp.minimum(scores, 0.0) - soft
    stacked = jnp.concatenate(
        [log_keep[:, t * LANES : (t + 1) * LANES] for t in range(tiles)], axis=0
    )
    terms = jnp.concatenate(three_terms(stacked), axis=0)
    r = lax.broadcasted_iota(jnp.int32, (LANES, 2 * LANES), 0)
    s = lax.broadcasted_iota(jnp.int32, (LANES, 2 * LANES), 1)
    later = jnp.where((r > s) | (s >= LANES), 1.0, 0.0).astype(BF16)
    sums = jnp.dot(terms, later, preferred_element_type=F32)
    count = tiles * sequences
    sums = sums[:count] + sums[count : 2 * count] + sums[2 * count :]
    running = jnp.zeros((sequences, LANES), F32)
    suffixes = [None] * tiles
    for t in reversed(range(tiles)):
        block = sums[t * sequences : (t + 1) * sequences]
        suffixes[t] = block[:, :LANES] + running
        running = running + block[:, LANES:]
    suffix = jnp.concatenate(suffixes, axis=1)
    weights = jnp.where(usable, jnp.exp(log_gate + suffix), 0.0).astype(BF16)
    values = jnp.concatenate([values_ref[b] for b in range(sequences)], axis=1)
    products = jnp.dot(weights, values, preferred_element_type=F32)
    out = jnp.zeros((sequences, head_size), F32)
    for b in range(sequences):
        out = jnp.where(row == b, products[:, b * head_size : (b + 1) * head_size], out)
    packed = jnp.concatenate([out, running], axis=1)
    for device in range(packed_ref.shape[0]):
        packed_ref[device] = packed


def output_kernel(order, every_ref, side_ref, w_out_ref, part_ref):
    size, sequences, _ = every_ref.shape
    place = {device: index for index, device in enumerate(order)}
    later_sum = jnp.zeros((sequences, LANES), F32)
    attended = jnp.zeros((sequences, LANES), F32)
    for n in reversed(range(size)):
        d = place[n]
        attended = attended + every_ref[d, :, :LANES] * jnp.exp(later_sum)
        later_sum = later_sum + every_ref[d, :, LANES:]
    mean_sq = jnp.mean(attended * attended, axis=1, keepdims=True)
    gain = side_ref[sequences + 1 : sequences + 2, :]
    normed = (attended * lax.rsqrt(mean_sq + EPS) * gain).astype(BF16)
    part = jnp.dot(normed, w_out_ref[...], preferred_element_type=F32)
    part_ref[...] = part.astype(BF16)


def mix_kernel(*refs):
    parts = [ref[...].astype(F32) for ref in refs[:-1]]
    while len(parts) > 1:
        parts = [parts[i] + parts[i + 1] for i in range(0, len(parts), 2)]
    refs[-1][...] = parts[0].astype(BF16)


def led_by(leader, size):
    return [leader] + [i for i in range(size) if i != leader]


def shards(
    tokens, in_gain, w_query, score_bias, cache_keys, cache_values, lengths, head_gain, w_out
):
    sequences, features = tokens.shape
    head_width = cache_keys.shape[2]
    assert score_bias.shape[0] == 1 and head_width == LANES
    kv_size = lax.axis_size("kv")
    tp_size = lax.axis_size("tp")
    columns = w_out.shape[1]
    seed = pl.pallas_call(
        opening_kernel,
        out_shape=pltpu.VMEM((sequences, LANES), F32),
        out_specs=VMEM,
        compiler_params=pltpu.CompilerParams(vmem_limit_bytes=1 << 20),
        cost_estimate=pl.CostEstimate(flops=1 << 33, bytes_accessed=128 << 20, transcendentals=0),
    )()
    packed, side = pl.pallas_call(
        query_kernel,
        out_shape=(
            jax.ShapeDtypeStruct((kv_size, sequences, 2 * LANES), F32),
            jax.ShapeDtypeStruct((2 * sequences, LANES), F32),
        ),
        in_specs=[VMEM] * 7,
        out_specs=(VMEM, VMEM),
        compiler_params=pltpu.CompilerParams(vmem_limit_bytes=4 << 20),
        cost_estimate=pl.CostEstimate(flops=1 << 33, bytes_accessed=128 << 20, transcendentals=0),
    )(seed, tokens, in_gain[None], w_query, score_bias[None], lengths[None], head_gain[None])
    first = led_by(kv_size * 5 // 8, kv_size)
    gathered = lax.all_to_all(packed, "kv", 0, 0, axis_index_groups=[first], tiled=False)
    packed = pl.pallas_call(
        functools.partial(attention_kernel, features * kv_size),
        out_shape=jax.ShapeDtypeStruct((kv_size, sequences, 2 * LANES), F32),
        in_specs=[VMEM, VMEM, VMEM, VMEM],
        out_specs=VMEM,
        compiler_params=pltpu.CompilerParams(vmem_limit_bytes=24 << 20),
    )(gathered, side, cache_keys, cache_values)
    second = led_by(kv_size * 5 // 8, kv_size)
    every = lax.all_to_all(packed, "kv", 0, 0, axis_index_groups=[second], tiled=False)
    part = pl.pallas_call(
        functools.partial(output_kernel, second),
        out_shape=jax.ShapeDtypeStruct((sequences, columns), BF16),
        in_specs=[VMEM] * 3,
        out_specs=VMEM,
        compiler_params=pltpu.CompilerParams(vmem_limit_bytes=4 << 20),
    )(every, side, w_out)
    parts = {0: part}
    for shift in range(tp_size - 1, 0, -1):
        parts[shift] = lax.ppermute(part, "tp", [(i, i ^ shift) for i in range(tp_size)])
    return pl.pallas_call(
        mix_kernel,
        out_shape=jax.ShapeDtypeStruct((sequences, columns), BF16),
        in_specs=[VMEM] * tp_size,
        out_specs=VMEM,
        compiler_params=pltpu.CompilerParams(vmem_limit_bytes=4 << 20),
    )(*[parts[shift] for shift in range(tp_size)])


def solution(mesh):
    return jax.shard_map(
        shards,
        mesh=mesh,
        in_specs=(
            P(None, "kv"),
            P("kv"),
            P("kv", "tp"),
            P("tp"),
            P(None, "kv", "tp"),
            P(None, "kv", "tp"),
            P(),
            P("tp"),
            P("tp", "kv"),
        ),
        out_specs=P(None, "kv"),
        check_vma=False,
    )
```

```python
import functools

import jax
import jax.numpy as jnp
from jax import lax
from jax.experimental import pallas as pl
from jax.experimental.pallas import tpu as pltpu
from jax.sharding import PartitionSpec as P


EPS = 1e-06
LANES = 128
VMEM = pl.BlockSpec(memory_space=pltpu.VMEM)
SMEM = pl.BlockSpec(memory_space=pltpu.SMEM)
HBM = pl.BlockSpec(memory_space=pltpu.HBM)
F32 = jnp.float32
BF16 = jnp.bfloat16


def three_terms(value):
    high = value.astype(BF16)
    rest = value - high.astype(F32)
    middle = rest.astype(BF16)
    low = (rest - middle.astype(F32)).astype(BF16)
    return high, middle, low


def opening_kernel(seed_ref):
    seed_ref[...] = jnp.zeros_like(seed_ref)


def query_kernel(
    seed_ref, tokens_ref, in_gain_ref, w_ref, bias_ref, lengths_ref, head_gain_ref, w_out_ref,
    packed_ref, side_ref, block_ref,
):
    block_ref[...] = w_out_ref[...]
    as_float = tokens_ref[...].astype(F32)
    sequences = as_float.shape[0]
    gained = (as_float * in_gain_ref[...]).astype(BF16)
    squares = jnp.sum(as_float * as_float, axis=1, keepdims=True)
    squares = jnp.broadcast_to(squares, (sequences, LANES))
    row = lax.broadcasted_iota(jnp.int32, (2 * sequences, LANES), 0)
    side = jnp.where(row == sequences, bias_ref[...], 0.0)
    side = jnp.where(row == sequences + 1, head_gain_ref[...], side)
    lengths = lengths_ref[...].astype(F32)
    own = lax.broadcasted_iota(jnp.int32, (2 * sequences, sequences), 0)
    own = own == lax.broadcasted_iota(jnp.int32, (2 * sequences, sequences), 1)
    lengths = jnp.sum(jnp.where(own, lengths, 0.0), axis=1, keepdims=True)
    side = jnp.where(row < sequences, lengths, side)
    side_ref[...] = side + seed_ref[:1]
    partial_value = jnp.dot(gained, w_ref[...], preferred_element_type=F32)
    packed = jnp.concatenate([partial_value, squares], axis=1)
    for device in range(packed_ref.shape[0]):
        packed_ref[device] = packed


def attention_kernel(width, gathered_ref, side_ref, keys_ref, values_ref, packed_ref):
    sequences, local_len, head_size = keys_ref.shape
    tiles = local_len // LANES
    gathered = jnp.sum(gathered_ref[...], axis=0)
    row_scale = lax.rsqrt(gathered[:, head_size:] / width + EPS)
    queries = gathered[:, :head_size] * row_scale
    row = lax.broadcasted_iota(jnp.int32, (sequences, head_size), 0)
    lane = lax.broadcasted_iota(jnp.int32, (sequences, LANES), 1)
    spread = jnp.concatenate(
        [jnp.where(row == b, queries, 0.0) for b in range(sequences)], axis=1
    ).astype(BF16)
    keys = jnp.concatenate([keys_ref[b] for b in range(sequences)], axis=1)
    scores = lax.dot_general(
        spread, keys, (((1,), (1,)), ((), ())), preferred_element_type=F32
    )
    bias = side_ref[sequences : sequences + 1, :]
    bias = jnp.concatenate([bias] * tiles, axis=1)
    scores = scores * head_size ** (-0.5) + bias
    here = lax.axis_index("kv") * local_len
    limit = side_ref[:sequences, :].astype(jnp.int32) - here
    usable = jnp.concatenate([lane + t * LANES < limit for t in range(tiles)], axis=1)
    soft = jnp.log1p(jnp.exp(-jnp.abs(scores)))
    log_keep = jnp.where(usable, -jnp.maximum(scores, 0.0) - soft, 0.0)
    log_gate = jnp.minimum(scores, 0.0) - soft
    stacked = jnp.concatenate(
        [log_keep[:, t * LANES : (t + 1) * LANES] for t in range(tiles)], axis=0
    )
    terms = jnp.concatenate(three_terms(stacked), axis=0)
    r = lax.broadcasted_iota(jnp.int32, (LANES, 2 * LANES), 0)
    s = lax.broadcasted_iota(jnp.int32, (LANES, 2 * LANES), 1)
    later = jnp.where((r > s) | (s >= LANES), 1.0, 0.0).astype(BF16)
    sums = jnp.dot(terms, later, preferred_element_type=F32)
    count = tiles * sequences
    sums = sums[:count] + sums[count : 2 * count] + sums[2 * count :]
    running = jnp.zeros((sequences, LANES), F32)
    suffixes = [None] * tiles
    for t in reversed(range(tiles)):
        block = sums[t * sequences : (t + 1) * sequences]
        suffixes[t] = block[:, :LANES] + running
        running = running + block[:, LANES:]
    suffix = jnp.concatenate(suffixes, axis=1)
    weights = jnp.where(usable, jnp.exp(log_gate + suffix), 0.0).astype(BF16)
    values = jnp.concatenate([values_ref[b] for b in range(sequences)], axis=1)
    products = jnp.dot(weights, values, preferred_element_type=F32)
    out = jnp.zeros((sequences, head_size), F32)
    for b in range(sequences):
        out = jnp.where(row == b, products[:, b * head_size : (b + 1) * head_size], out)
    gains = three_terms(side_ref[sequences + 1 : sequences + 2, :])
    extra = jnp.zeros((sequences, LANES), F32)
    for i, term in enumerate(three_terms(running)):
        spot = jnp.where(lane == row + i * sequences, term.astype(F32), 0.0)
        spot = jnp.sum(spot, axis=0, keepdims=True)
        extra = extra + jnp.where(row == 0, spot, 0.0)
    for i, term in enumerate(gains):
        extra = jnp.where(row == 1 + i, term.astype(F32), extra)
    packed = jnp.concatenate([out, extra], axis=0).astype(BF16)
    for device in range(packed_ref.shape[0]):
        packed_ref[device] = packed


def output_kernel(kv_order, every_ref, own_ref, partner_ref, pair_ref):
    sequences, _ = pair_ref.shape
    row = lax.broadcasted_iota(jnp.int32, (sequences, LANES), 0)
    lane = lax.broadcasted_iota(jnp.int32, (sequences, LANES), 1)
    spot = (lane % sequences == row) & (lane < 3 * sequences)
    parity = lax.axis_index("tp") % 2
    size = len(kv_order)
    blocks = [every_ref[2 * k + 1 - parity] for k in range(size)]
    blocks += [every_ref[2 * k + parity] for k in range(size)]
    extras = [block[sequences:, :].astype(F32) for block in blocks]
    terms = jnp.concatenate(
        [jnp.where(spot, extra[:1], 0.0) for extra in extras], axis=0
    ).astype(BF16)
    totals = jnp.dot(terms, jnp.ones((LANES, LANES), BF16), preferred_element_type=F32)
    parts = []
    for head, w_out_ref in enumerate((own_ref, partner_ref)):
        later_sum = jnp.zeros((sequences, LANES), F32)
        attended = jnp.zeros((sequences, LANES), F32)
        for n in reversed(range(size)):
            d = head * size + kv_order.index(n)
            out = blocks[d][:sequences, :].astype(F32)
            attended = attended + out * jnp.exp(later_sum)
            later_sum = later_sum + totals[d * sequences : (d + 1) * sequences]
        mean_sq = jnp.mean(attended * attended, axis=1, keepdims=True)
        extra = extras[head * size]
        gain = extra[1:2] + extra[2:3] + extra[3:4]
        normed = (attended * lax.rsqrt(mean_sq + EPS) * gain).astype(BF16)
        part = jnp.dot(normed, w_out_ref[...], preferred_element_type=F32)
        parts.append(part.astype(BF16).astype(F32))
    pair_ref[...] = parts[0] + parts[1]


def mix_kernel(*refs):
    parts = [ref[...] for ref in refs[:-1]]
    while len(parts) > 1:
        parts = [parts[i] + parts[i + 1] for i in range(0, len(parts), 2)]
    refs[-1][...] = parts[0].astype(BF16)


def led_by(leader, size):
    return [leader] + [i for i in range(size) if i != leader]


def shards(
    tokens, in_gain, w_query, score_bias, cache_keys, cache_values, lengths, head_gain, w_out
):
    sequences, features = tokens.shape
    head_width = cache_keys.shape[2]
    assert score_bias.shape[0] == 1 and head_width == LANES
    kv_size = lax.axis_size("kv")
    tp_size = lax.axis_size("tp")
    columns = w_out.shape[1]
    pairs = tp_size // 2
    assert tp_size % 2 == 0 and pairs & (pairs - 1) == 0
    seed = pl.pallas_call(
        opening_kernel,
        out_shape=pltpu.VMEM((sequences, LANES), F32),
        out_specs=VMEM,
        compiler_params=pltpu.CompilerParams(vmem_limit_bytes=1 << 20),
        cost_estimate=pl.CostEstimate(
            flops=1 << 33, bytes_accessed=128 << 20, transcendentals=0
        ),
    )()
    packed, side, block = pl.pallas_call(
        query_kernel,
        out_shape=(
            jax.ShapeDtypeStruct((kv_size, sequences, 2 * LANES), F32),
            jax.ShapeDtypeStruct((2 * sequences, LANES), F32),
            jax.ShapeDtypeStruct(w_out.shape, BF16),
        ),
        in_specs=[VMEM] * 8,
        out_specs=(VMEM,) * 3,
        compiler_params=pltpu.CompilerParams(vmem_limit_bytes=4 << 20),
        cost_estimate=pl.CostEstimate(
            flops=1 << 33, bytes_accessed=128 << 20, transcendentals=0
        ),
    )(seed, tokens, in_gain[None], w_query, score_bias[None], lengths[None], head_gain[None], w_out)
    partner = lax.ppermute(block, "tp", [(i, i ^ 1) for i in range(tp_size)])
    first = led_by(kv_size * 5 // 8, kv_size)
    gathered = lax.all_to_all(packed, "kv", 0, 0, axis_index_groups=[first], tiled=False)
    packed = pl.pallas_call(
        functools.partial(attention_kernel, features * kv_size),
        out_shape=jax.ShapeDtypeStruct((2 * kv_size, 2 * sequences, LANES), BF16),
        in_specs=[VMEM, VMEM, VMEM, VMEM],
        out_specs=VMEM,
        compiler_params=pltpu.CompilerParams(vmem_limit_bytes=24 << 20),
    )(gathered, side, cache_keys, cache_values)
    packed, partner = lax.optimization_barrier((packed, partner))
    groups = [
        [n * tp_size + 2 * pair + parity for n in first for parity in (1, 0)]
        for pair in range(pairs)
    ]
    every = lax.all_to_all(
        packed, ("kv", "tp"), 0, 0, axis_index_groups=groups, tiled=False
    )
    pair_sum = pl.pallas_call(
        functools.partial(output_kernel, first),
        out_shape=jax.ShapeDtypeStruct((sequences, columns), F32),
        in_specs=[VMEM] * 3,
        out_specs=VMEM,
        compiler_params=pltpu.CompilerParams(vmem_limit_bytes=4 << 20),
    )(every, block, partner)
    sums = [pair_sum]
    for shift in range(1, pairs):
        moves = [(i, i ^ (2 * shift + 1)) for i in range(tp_size)]
        sums.append(lax.ppermute(pair_sum, "tp", moves))
    return pl.pallas_call(
        mix_kernel,
        out_shape=jax.ShapeDtypeStruct((sequences, columns), BF16),
        in_specs=[VMEM] * pairs,
        out_specs=VMEM,
        compiler_params=pltpu.CompilerParams(vmem_limit_bytes=4 << 20),
    )(*sums)


def solution(mesh):
    return jax.shard_map(
        shards,
        mesh=mesh,
        in_specs=(
            P(None, "kv"),
            P("kv"),
            P("kv", "tp"),
            P("tp"),
            P(None, "kv", "tp"),
            P(None, "kv", "tp"),
            P(),
            P("tp"),
            P("tp", "kv"),
        ),
        out_specs=P(None, "kv"),
        check_vma=False,
    )
```

```python
import functools

import jax
import jax.numpy as jnp
from jax import lax
from jax.experimental import pallas as pl
from jax.experimental.pallas import tpu as pltpu
from jax.sharding import PartitionSpec as P


EPS = 1e-06
LANES = 128
VMEM = pl.BlockSpec(memory_space=pltpu.VMEM)
SMEM = pl.BlockSpec(memory_space=pltpu.SMEM)
HBM = pl.BlockSpec(memory_space=pltpu.HBM)
F32 = jnp.float32
BF16 = jnp.bfloat16


def three_terms(value):
    high = value.astype(BF16)
    rest = value - high.astype(F32)
    middle = rest.astype(BF16)
    low = (rest - middle.astype(F32)).astype(BF16)
    return high, middle, low


def opening_kernel(seed_ref):
    seed_ref[...] = jnp.zeros_like(seed_ref)


def query_kernel(
    seed_ref, tokens_ref, in_gain_ref, w_ref, bias_ref, lengths_ref, head_gain_ref, w_out_ref,
    packed_ref, side_ref, block_ref,
):
    rows, columns = w_out_ref.shape
    if columns < block_ref.shape[1]:
        block_ref[...] = jnp.zeros_like(block_ref)
    block_ref[:rows, :columns] = w_out_ref[...]
    high, middle, low = three_terms(head_gain_ref[...])
    line = lax.broadcasted_iota(jnp.int32, (16, rows), 0)
    gains = jnp.where(line == 0, high.astype(F32), 0.0)
    gains = jnp.where(line == 1, middle.astype(F32), gains)
    gains = jnp.where(line == 2, low.astype(F32), gains)
    block_ref[rows : rows + 16, :rows] = gains.astype(BF16)
    as_float = tokens_ref[...].astype(F32)
    sequences = as_float.shape[0]
    gained = (as_float * in_gain_ref[...]).astype(BF16)
    squares = jnp.sum(as_float * as_float, axis=1, keepdims=True)
    row = lax.broadcasted_iota(jnp.int32, (2 * sequences, LANES), 0)
    side = jnp.where(row == sequences, bias_ref[...], 0.0)
    lengths = lengths_ref[...].astype(F32)
    own = lax.broadcasted_iota(jnp.int32, (2 * sequences, sequences), 0)
    own = own == lax.broadcasted_iota(jnp.int32, (2 * sequences, sequences), 1)
    lengths = jnp.sum(jnp.where(own, lengths, 0.0), axis=1, keepdims=True)
    side = jnp.where(row < sequences, lengths, side)
    side_ref[...] = side + seed_ref[:1]
    partial_value = jnp.dot(gained, w_ref[...], preferred_element_type=F32)
    quarters = sequences // 2
    lane = lax.broadcasted_iota(jnp.int32, (2, LANES), 1)
    spread = jnp.zeros((2, LANES), F32)
    for c in range(quarters):
        spread = jnp.where(lane == c, squares[2 * c : 2 * c + 2], spread)
    packed = [partial_value[2 * c : 2 * c + 2] for c in range(quarters)] + [spread]
    packed = jnp.concatenate(packed, axis=1)
    for device in range(packed_ref.shape[0]):
        packed_ref[device] = packed


def attention_kernel(width, gathered_ref, side_ref, keys_ref, values_ref, packed_ref):
    sequences, local_len, head_size = keys_ref.shape
    tiles = local_len // LANES
    gathered = jnp.sum(gathered_ref[...], axis=0)
    quarters = sequences // 2
    row_scale = lax.rsqrt(gathered[:, quarters * head_size :] / width + EPS)
    queries = jnp.concatenate(
        [
            gathered[:, c * head_size : (c + 1) * head_size] * row_scale[:, c : c + 1]
            for c in range(quarters)
        ],
        axis=0,
    )
    row = lax.broadcasted_iota(jnp.int32, (sequences, head_size), 0)
    lane = lax.broadcasted_iota(jnp.int32, (sequences, LANES), 1)
    spread = jnp.concatenate(
        [jnp.where(row == b, queries, 0.0) for b in range(sequences)], axis=1
    ).astype(BF16)
    keys = jnp.concatenate([keys_ref[b] for b in range(sequences)], axis=1)
    scores = lax.dot_general(
        spread, keys, (((1,), (1,)), ((), ())), preferred_element_type=F32
    )
    bias = side_ref[sequences : sequences + 1, :]
    bias = jnp.concatenate([bias] * tiles, axis=1)
    scores = scores * head_size ** (-0.5) + bias
    here = lax.axis_index("kv") * local_len
    limit = side_ref[:sequences, :].astype(jnp.int32) - here
    usable = jnp.concatenate([lane + t * LANES < limit for t in range(tiles)], axis=1)
    soft = jnp.log1p(jnp.exp(-jnp.abs(scores)))
    log_keep = jnp.where(usable, -jnp.maximum(scores, 0.0) - soft, 0.0)
    log_gate = jnp.minimum(scores, 0.0) - soft
    stacked = jnp.concatenate(
        [log_keep[:, t * LANES : (t + 1) * LANES] for t in range(tiles)], axis=0
    )
    terms = jnp.concatenate(three_terms(stacked), axis=0)
    r = lax.broadcasted_iota(jnp.int32, (LANES, 2 * LANES), 0)
    s = lax.broadcasted_iota(jnp.int32, (LANES, 2 * LANES), 1)
    later = jnp.where((r > s) | (s >= LANES), 1.0, 0.0).astype(BF16)
    sums = jnp.dot(terms, later, preferred_element_type=F32)
    count = tiles * sequences
    sums = sums[:count] + sums[count : 2 * count] + sums[2 * count :]
    running = jnp.zeros((sequences, LANES), F32)
    suffixes = [None] * tiles
    for t in reversed(range(tiles)):
        block = sums[t * sequences : (t + 1) * sequences]
        suffixes[t] = block[:, :LANES] + running
        running = running + block[:, LANES:]
    suffix = jnp.concatenate(suffixes, axis=1)
    weights = jnp.where(usable, jnp.exp(log_gate + suffix), 0.0).astype(BF16)
    values = jnp.concatenate([values_ref[b] for b in range(sequences)], axis=1)
    products = jnp.dot(weights, values, preferred_element_type=F32)
    out = jnp.zeros((sequences, head_size), F32)
    for b in range(sequences):
        out = jnp.where(row == b, products[:, b * head_size : (b + 1) * head_size], out)
    high = running.astype(BF16).astype(F32)
    extra = jnp.where(lane < LANES // 2, high, running - high)
    packed = jnp.concatenate([out, extra], axis=0).astype(BF16)
    for device in range(packed_ref.shape[0]):
        packed_ref[device] = packed


def output_kernel(kv_order, every_ref, own_ref, partner_ref, pair_ref):
    sequences, columns = pair_ref.shape
    parity = lax.axis_index("tp") % 2
    size = len(kv_order)
    parts = []
    for block_ref, offset in ((own_ref, 1 - parity), (partner_ref, parity)):
        later_sum = jnp.zeros((sequences, LANES), F32)
        attended = jnp.zeros((sequences, LANES), F32)
        for n in reversed(range(size)):
            packed = every_ref[2 * kv_order.index(n) + offset].astype(F32)
            halves = packed[sequences:]
            attended = attended + packed[:sequences] * jnp.exp(later_sum)
            later_sum = later_sum + (halves + pltpu.roll(halves, LANES // 2, 1))
        mean_sq = jnp.mean(attended * attended, axis=1, keepdims=True)
        gain = block_ref[LANES : LANES + 16, :LANES].astype(F32)
        gain = gain[0:1] + gain[1:2] + gain[2:3]
        normed = (attended * lax.rsqrt(mean_sq + EPS) * gain).astype(BF16)
        part = jnp.dot(normed, block_ref[:LANES, :columns], preferred_element_type=F32)
        parts.append(part.astype(BF16).astype(F32))
    pair_ref[...] = parts[0] + parts[1]


def mix_kernel(*refs):
    parts = [ref[...] for ref in refs[:-1]]
    while len(parts) > 1:
        parts = [parts[i] + parts[i + 1] for i in range(0, len(parts), 2)]
    refs[-1][...] = parts[0].astype(BF16)


def led_by(leader, size):
    return [leader] + [i for i in range(size) if i != leader]


def shards(
    tokens, in_gain, w_query, score_bias, cache_keys, cache_values, lengths, head_gain, w_out
):
    sequences, features = tokens.shape
    head_width = cache_keys.shape[2]
    assert score_bias.shape[0] == 1 and head_width == LANES
    kv_size = lax.axis_size("kv")
    tp_size = lax.axis_size("tp")
    columns = w_out.shape[1]
    pairs = tp_size // 2
    assert tp_size % 2 == 0 and pairs & (pairs - 1) == 0
    seed = pl.pallas_call(
        opening_kernel,
        out_shape=pltpu.VMEM((sequences, LANES), F32),
        out_specs=VMEM,
        compiler_params=pltpu.CompilerParams(vmem_limit_bytes=1 << 20),
        cost_estimate=pl.CostEstimate(
            flops=1 << 33, bytes_accessed=128 << 20, transcendentals=0
        ),
    )()
    packed, side, block = pl.pallas_call(
        query_kernel,
        out_shape=(
            jax.ShapeDtypeStruct((kv_size, 2, (sequences // 2 + 1) * LANES), F32),
            jax.ShapeDtypeStruct((2 * sequences, LANES), F32),
            jax.ShapeDtypeStruct((head_width + 16, max(columns, LANES)), BF16),
        ),
        in_specs=[VMEM] * 8,
        out_specs=(VMEM,) * 3,
        compiler_params=pltpu.CompilerParams(vmem_limit_bytes=4 << 20),
        cost_estimate=pl.CostEstimate(
            flops=1 << 33, bytes_accessed=128 << 20, transcendentals=0
        ),
    )(seed, tokens, in_gain[None], w_query, score_bias[None], lengths[None], head_gain[None], w_out)
    partner = lax.ppermute(block, "tp", [(i, i ^ 1) for i in range(tp_size)])
    first = led_by(kv_size * 5 // 8, kv_size)
    gathered = lax.all_to_all(packed, "kv", 0, 0, axis_index_groups=[first], tiled=False)
    packed = pl.pallas_call(
        functools.partial(attention_kernel, features * kv_size),
        out_shape=jax.ShapeDtypeStruct((2 * kv_size, 2 * sequences, LANES), BF16),
        in_specs=[VMEM, VMEM, VMEM, VMEM],
        out_specs=VMEM,
        compiler_params=pltpu.CompilerParams(vmem_limit_bytes=24 << 20),
    )(gathered, side, cache_keys, cache_values)
    packed, partner = lax.optimization_barrier((packed, partner))
    groups = [
        [n * tp_size + 2 * pair + parity for n in first for parity in (1, 0)]
        for pair in range(pairs)
    ]
    every = lax.all_to_all(
        packed, ("kv", "tp"), 0, 0, axis_index_groups=groups, tiled=False
    )
    pair_sum = pl.pallas_call(
        functools.partial(output_kernel, first),
        out_shape=jax.ShapeDtypeStruct((sequences, columns), F32),
        in_specs=[VMEM] * 3,
        out_specs=VMEM,
        compiler_params=pltpu.CompilerParams(vmem_limit_bytes=4 << 20),
    )(every, block, partner)
    sums = [pair_sum]
    for shift in range(1, pairs):
        moves = [(i, i ^ (2 * shift + 1)) for i in range(tp_size)]
        sums.append(lax.ppermute(pair_sum, "tp", moves))
    return pl.pallas_call(
        mix_kernel,
        out_shape=jax.ShapeDtypeStruct((sequences, columns), BF16),
        in_specs=[VMEM] * pairs,
        out_specs=VMEM,
        compiler_params=pltpu.CompilerParams(vmem_limit_bytes=4 << 20),
    )(*sums)


def solution(mesh):
    return jax.shard_map(
        shards,
        mesh=mesh,
        in_specs=(
            P(None, "kv"),
            P("kv"),
            P("kv", "tp"),
            P("tp"),
            P(None, "kv", "tp"),
            P(None, "kv", "tp"),
            P(),
            P("tp"),
            P("tp", "kv"),
        ),
        out_specs=P(None, "kv"),
        check_vma=False,
    )
```

```python
import functools

import jax
import jax.numpy as jnp
from jax import lax
from jax.experimental import pallas as pl
from jax.experimental.pallas import tpu as pltpu
from jax.sharding import PartitionSpec as P


EPS = 1e-06
LANES = 128
VMEM = pl.BlockSpec(memory_space=pltpu.VMEM)
SMEM = pl.BlockSpec(memory_space=pltpu.SMEM)
HBM = pl.BlockSpec(memory_space=pltpu.HBM)
F32 = jnp.float32
BF16 = jnp.bfloat16


def three_terms(value):
    high = value.astype(BF16)
    rest = value - high.astype(F32)
    middle = rest.astype(BF16)
    low = (rest - middle.astype(F32)).astype(BF16)
    return high, middle, low


def opening_kernel(seed_ref):
    seed_ref[...] = jnp.zeros_like(seed_ref)


def query_kernel(
    seed_ref, tokens_ref, in_gain_ref, w_ref, bias_ref, lengths_ref, head_gain_ref, w_out_ref,
    packed_ref, side_ref, block_ref,
):
    rows, columns = w_out_ref.shape
    if columns < block_ref.shape[1]:
        block_ref[...] = jnp.zeros_like(block_ref)
    block_ref[:rows, :columns] = w_out_ref[...]
    high, middle, low = three_terms(head_gain_ref[...])
    line = lax.broadcasted_iota(jnp.int32, (16, rows), 0)
    gains = jnp.where(line == 0, high.astype(F32), 0.0)
    gains = jnp.where(line == 1, middle.astype(F32), gains)
    gains = jnp.where(line == 2, low.astype(F32), gains)
    block_ref[rows : rows + 16, :rows] = gains.astype(BF16)
    as_float = tokens_ref[...].astype(F32)
    sequences = as_float.shape[0]
    gained = (as_float * in_gain_ref[...]).astype(BF16)
    squares = jnp.sum(as_float * as_float, axis=1, keepdims=True)
    row = lax.broadcasted_iota(jnp.int32, (2 * sequences, LANES), 0)
    side = jnp.where(row == sequences, bias_ref[...], 0.0)
    lengths = lengths_ref[...].astype(F32)
    own = lax.broadcasted_iota(jnp.int32, (2 * sequences, sequences), 0)
    own = own == lax.broadcasted_iota(jnp.int32, (2 * sequences, sequences), 1)
    lengths = jnp.sum(jnp.where(own, lengths, 0.0), axis=1, keepdims=True)
    side = jnp.where(row < sequences, lengths, side)
    side_ref[...] = side + seed_ref[:1]
    partial_value = jnp.dot(gained, w_ref[...], preferred_element_type=F32)
    quarters = sequences // 2
    lane = lax.broadcasted_iota(jnp.int32, (2, LANES), 1)
    spread = jnp.zeros((2, LANES), F32)
    for c in range(quarters):
        spread = jnp.where(lane == c, squares[2 * c : 2 * c + 2], spread)
    packed = [partial_value[2 * c : 2 * c + 2] for c in range(quarters)] + [spread]
    packed = jnp.concatenate(packed, axis=1)
    for device in range(packed_ref.shape[0]):
        packed_ref[device] = packed


def attention_kernel(width, gathered_ref, side_ref, keys_ref, values_ref, packed_ref):
    sequences, local_len, head_size = keys_ref.shape
    tiles = local_len // LANES
    parity = lax.axis_index("tp") % 2
    gathered = gathered_ref[1 - parity]
    for k in range(1, gathered_ref.shape[0] // 2):
        gathered = gathered + gathered_ref[2 * k + 1 - parity]
    quarters = sequences // 2
    row_scale = lax.rsqrt(gathered[:, quarters * head_size :] / width + EPS)
    queries = jnp.concatenate(
        [
            gathered[:, c * head_size : (c + 1) * head_size] * row_scale[:, c : c + 1]
            for c in range(quarters)
        ],
        axis=0,
    )
    row = lax.broadcasted_iota(jnp.int32, (sequences, head_size), 0)
    lane = lax.broadcasted_iota(jnp.int32, (sequences, LANES), 1)
    spread = jnp.concatenate(
        [jnp.where(row == b, queries, 0.0) for b in range(sequences)], axis=1
    ).astype(BF16)
    keys = jnp.concatenate([keys_ref[b] for b in range(sequences)], axis=1)
    scores = lax.dot_general(
        spread, keys, (((1,), (1,)), ((), ())), preferred_element_type=F32
    )
    bias = side_ref[sequences : sequences + 1, :]
    bias = jnp.concatenate([bias] * tiles, axis=1)
    scores = scores * head_size ** (-0.5) + bias
    here = lax.axis_index("kv") * local_len
    limit = side_ref[:sequences, :].astype(jnp.int32) - here
    usable = jnp.concatenate([lane + t * LANES < limit for t in range(tiles)], axis=1)
    soft = jnp.log1p(jnp.exp(-jnp.abs(scores)))
    log_keep = jnp.where(usable, -jnp.maximum(scores, 0.0) - soft, 0.0)
    log_gate = jnp.minimum(scores, 0.0) - soft
    stacked = jnp.concatenate(
        [log_keep[:, t * LANES : (t + 1) * LANES] for t in range(tiles)], axis=0
    )
    terms = jnp.concatenate(three_terms(stacked), axis=0)
    r = lax.broadcasted_iota(jnp.int32, (LANES, 2 * LANES), 0)
    s = lax.broadcasted_iota(jnp.int32, (LANES, 2 * LANES), 1)
    later = jnp.where((r > s) | (s >= LANES), 1.0, 0.0).astype(BF16)
    sums = jnp.dot(terms, later, preferred_element_type=F32)
    count = tiles * sequences
    sums = sums[:count] + sums[count : 2 * count] + sums[2 * count :]
    running = jnp.zeros((sequences, LANES), F32)
    suffixes = [None] * tiles
    for t in reversed(range(tiles)):
        block = sums[t * sequences : (t + 1) * sequences]
        suffixes[t] = block[:, :LANES] + running
        running = running + block[:, LANES:]
    suffix = jnp.concatenate(suffixes, axis=1)
    weights = jnp.where(usable, jnp.exp(log_gate + suffix), 0.0).astype(BF16)
    values = jnp.concatenate([values_ref[b] for b in range(sequences)], axis=1)
    products = jnp.dot(weights, values, preferred_element_type=F32)
    out = jnp.zeros((sequences, head_size), F32)
    for b in range(sequences):
        out = jnp.where(row == b, products[:, b * head_size : (b + 1) * head_size], out)
    high = running.astype(BF16).astype(F32)
    extra = jnp.where(lane < LANES // 2, high, running - high)
    packed = jnp.concatenate([out, extra], axis=0).astype(BF16)
    for device in range(packed_ref.shape[0]):
        packed_ref[device] = packed


def output_kernel(kv_order, every_ref, own_ref, partner_ref, pair_ref):
    sequences, columns = pair_ref.shape
    parity = lax.axis_index("tp") % 2
    size = len(kv_order)
    parts = []
    for block_ref, offset in ((own_ref, 1 - parity), (partner_ref, parity)):
        later_sum = jnp.zeros((sequences, LANES), F32)
        attended = jnp.zeros((sequences, LANES), F32)
        for n in reversed(range(size)):
            packed = every_ref[2 * kv_order.index(n) + offset].astype(F32)
            halves = packed[sequences:]
            attended = attended + packed[:sequences] * jnp.exp(later_sum)
            later_sum = later_sum + (halves + pltpu.roll(halves, LANES // 2, 1))
        mean_sq = jnp.mean(attended * attended, axis=1, keepdims=True)
        gain = block_ref[LANES : LANES + 16, :LANES].astype(F32)
        gain = gain[0:1] + gain[1:2] + gain[2:3]
        normed = (attended * lax.rsqrt(mean_sq + EPS) * gain).astype(BF16)
        part = jnp.dot(normed, block_ref[:LANES, :columns], preferred_element_type=F32)
        parts.append(part.astype(BF16).astype(F32))
    pair_ref[...] = parts[0] + parts[1]


def mix_kernel(*refs):
    parts = [ref[...] for ref in refs[:-1]]
    while len(parts) > 1:
        parts = [parts[i] + parts[i + 1] for i in range(0, len(parts), 2)]
    refs[-1][...] = parts[0].astype(BF16)


def led_by(leader, size):
    return [leader] + [i for i in range(size) if i != leader]


def shards(
    tokens, in_gain, w_query, score_bias, cache_keys, cache_values, lengths, head_gain, w_out
):
    sequences, features = tokens.shape
    head_width = cache_keys.shape[2]
    assert score_bias.shape[0] == 1 and head_width == LANES
    kv_size = lax.axis_size("kv")
    tp_size = lax.axis_size("tp")
    columns = w_out.shape[1]
    pairs = tp_size // 2
    assert tp_size % 2 == 0 and pairs & (pairs - 1) == 0
    seed = pl.pallas_call(
        opening_kernel,
        out_shape=pltpu.VMEM((sequences, LANES), F32),
        out_specs=VMEM,
        compiler_params=pltpu.CompilerParams(vmem_limit_bytes=1 << 20),
        cost_estimate=pl.CostEstimate(
            flops=1 << 33, bytes_accessed=128 << 20, transcendentals=0
        ),
    )()
    packed, side, block = pl.pallas_call(
        query_kernel,
        out_shape=(
            jax.ShapeDtypeStruct((2 * kv_size, 2, (sequences // 2 + 1) * LANES), F32),
            jax.ShapeDtypeStruct((2 * sequences, LANES), F32),
            jax.ShapeDtypeStruct((head_width + 16, max(columns, LANES)), BF16),
        ),
        in_specs=[VMEM] * 8,
        out_specs=(VMEM,) * 3,
        compiler_params=pltpu.CompilerParams(vmem_limit_bytes=4 << 20),
        cost_estimate=pl.CostEstimate(
            flops=1 << 20, bytes_accessed=1 << 16, transcendentals=0
        ),
    )(seed, tokens, in_gain[None], w_query, score_bias[None], lengths[None], head_gain[None], w_out)
    partner = lax.ppermute(block, "tp", [(i, i ^ 1) for i in range(tp_size)])
    first = led_by(kv_size * 5 // 8, kv_size)
    groups = [
        [n * tp_size + 2 * pair + parity for n in first for parity in (1, 0)]
        for pair in range(pairs)
    ]
    gathered = lax.all_to_all(
        packed, ("kv", "tp"), 0, 0, axis_index_groups=groups, tiled=False
    )
    packed = pl.pallas_call(
        functools.partial(attention_kernel, features * kv_size),
        out_shape=jax.ShapeDtypeStruct((2 * kv_size, 2 * sequences, LANES), BF16),
        in_specs=[VMEM, VMEM, VMEM, VMEM],
        out_specs=VMEM,
        compiler_params=pltpu.CompilerParams(vmem_limit_bytes=24 << 20),
    )(gathered, side, cache_keys, cache_values)
    packed, partner = lax.optimization_barrier((packed, partner))
    groups = [
        [n * tp_size + 2 * pair + parity for n in first for parity in (1, 0)]
        for pair in range(pairs)
    ]
    every = lax.all_to_all(
        packed, ("kv", "tp"), 0, 0, axis_index_groups=groups, tiled=False
    )
    pair_sum = pl.pallas_call(
        functools.partial(output_kernel, first),
        out_shape=jax.ShapeDtypeStruct((sequences, columns), F32),
        in_specs=[VMEM] * 3,
        out_specs=VMEM,
        compiler_params=pltpu.CompilerParams(vmem_limit_bytes=4 << 20),
    )(every, block, partner)
    sums = [pair_sum]
    for shift in range(1, pairs):
        moves = [(i, i ^ (2 * shift + 1)) for i in range(tp_size)]
        sums.append(lax.ppermute(pair_sum, "tp", moves))
    return pl.pallas_call(
        mix_kernel,
        out_shape=jax.ShapeDtypeStruct((sequences, columns), BF16),
        in_specs=[VMEM] * pairs,
        out_specs=VMEM,
        compiler_params=pltpu.CompilerParams(vmem_limit_bytes=4 << 20),
    )(*sums)


def solution(mesh):
    return jax.shard_map(
        shards,
        mesh=mesh,
        in_specs=(
            P(None, "kv"),
            P("kv"),
            P("kv", "tp"),
            P("tp"),
            P(None, "kv", "tp"),
            P(None, "kv", "tp"),
            P(),
            P("tp"),
            P("tp", "kv"),
        ),
        out_specs=P(None, "kv"),
        check_vma=False,
    )
```

```python
import functools

import jax
import jax.numpy as jnp
from jax import lax
from jax.experimental import pallas as pl
from jax.experimental.pallas import tpu as pltpu
from jax.sharding import PartitionSpec as P


EPS = 1e-06
LANES = 128
VMEM = pl.BlockSpec(memory_space=pltpu.VMEM)
SMEM = pl.BlockSpec(memory_space=pltpu.SMEM)
HBM = pl.BlockSpec(memory_space=pltpu.HBM)
F32 = jnp.float32
BF16 = jnp.bfloat16


def three_terms(value):
    high = value.astype(BF16)
    rest = value - high.astype(F32)
    middle = rest.astype(BF16)
    low = (rest - middle.astype(F32)).astype(BF16)
    return high, middle, low


def opening_kernel(seed_ref):
    seed_ref[...] = jnp.zeros_like(seed_ref)


def query_kernel(
    seed_ref, tokens_ref, in_gain_ref, w_ref, bias_ref, lengths_ref, head_gain_ref, w_out_ref,
    packed_ref, side_ref, block_ref,
):
    rows, columns = w_out_ref.shape
    if columns < block_ref.shape[1]:
        block_ref[...] = jnp.zeros_like(block_ref)
    block_ref[:rows, :columns] = w_out_ref[...]
    high, middle, low = three_terms(head_gain_ref[...])
    line = lax.broadcasted_iota(jnp.int32, (16, rows), 0)
    gains = jnp.where(line == 0, high.astype(F32), 0.0)
    gains = jnp.where(line == 1, middle.astype(F32), gains)
    gains = jnp.where(line == 2, low.astype(F32), gains)
    block_ref[rows : rows + 16, :rows] = gains.astype(BF16)
    as_float = tokens_ref[...].astype(F32)
    sequences = as_float.shape[0]
    gained = (as_float * in_gain_ref[...]).astype(BF16)
    squares = jnp.sum(as_float * as_float, axis=1, keepdims=True)
    row = lax.broadcasted_iota(jnp.int32, (2 * sequences, LANES), 0)
    side = jnp.where(row == sequences, bias_ref[...], 0.0)
    lengths = lengths_ref[...].astype(F32)
    own = lax.broadcasted_iota(jnp.int32, (2 * sequences, sequences), 0)
    own = own == lax.broadcasted_iota(jnp.int32, (2 * sequences, sequences), 1)
    lengths = jnp.sum(jnp.where(own, lengths, 0.0), axis=1, keepdims=True)
    side = jnp.where(row < sequences, lengths, side)
    side_ref[...] = side + seed_ref[:1]
    partial_value = jnp.dot(gained, w_ref[...], preferred_element_type=F32)
    quarters = sequences // 2
    lane = lax.broadcasted_iota(jnp.int32, (2, LANES), 1)
    spread = jnp.zeros((2, LANES), F32)
    for c in range(quarters):
        spread = jnp.where(lane == c, squares[2 * c : 2 * c + 2], spread)
    packed = [partial_value[2 * c : 2 * c + 2] for c in range(quarters)] + [spread]
    packed = jnp.concatenate(packed, axis=1)
    for device in range(packed_ref.shape[0]):
        packed_ref[device] = packed


def attention_kernel(width, gathered_ref, side_ref, keys_ref, values_ref, packed_ref):
    sequences, local_len, head_size = keys_ref.shape
    tiles = local_len // LANES
    parity = lax.axis_index("tp") % 2
    gathered = gathered_ref[1 - parity]
    for k in range(1, gathered_ref.shape[0] // 2):
        gathered = gathered + gathered_ref[2 * k + 1 - parity]
    quarters = sequences // 2
    row_scale = lax.rsqrt(gathered[:, quarters * head_size :] / width + EPS)
    queries = jnp.concatenate(
        [
            gathered[:, c * head_size : (c + 1) * head_size] * row_scale[:, c : c + 1]
            for c in range(quarters)
        ],
        axis=0,
    )
    row = lax.broadcasted_iota(jnp.int32, (sequences, head_size), 0)
    lane = lax.broadcasted_iota(jnp.int32, (sequences, LANES), 1)
    spread = jnp.concatenate(
        [jnp.where(row == b, queries, 0.0) for b in range(sequences)], axis=1
    ).astype(BF16)
    keys = jnp.concatenate([keys_ref[b] for b in range(sequences)], axis=1)
    scores = lax.dot_general(
        spread, keys, (((1,), (1,)), ((), ())), preferred_element_type=F32
    )
    bias = side_ref[sequences : sequences + 1, :]
    bias = jnp.concatenate([bias] * tiles, axis=1)
    scores = scores * head_size ** (-0.5) + bias
    here = lax.axis_index("kv") * local_len
    limit = side_ref[:sequences, :].astype(jnp.int32) - here
    usable = jnp.concatenate([lane + t * LANES < limit for t in range(tiles)], axis=1)
    soft = jnp.log1p(jnp.exp(-jnp.abs(scores)))
    log_keep = jnp.where(usable, -jnp.maximum(scores, 0.0) - soft, 0.0)
    log_gate = jnp.minimum(scores, 0.0) - soft
    stacked = jnp.concatenate(
        [log_keep[:, t * LANES : (t + 1) * LANES] for t in range(tiles)], axis=0
    )
    terms = jnp.concatenate(three_terms(stacked), axis=0)
    r = lax.broadcasted_iota(jnp.int32, (LANES, 2 * LANES), 0)
    s = lax.broadcasted_iota(jnp.int32, (LANES, 2 * LANES), 1)
    later = jnp.where((r > s) | (s >= LANES), 1.0, 0.0).astype(BF16)
    sums = jnp.dot(terms, later, preferred_element_type=F32)
    count = tiles * sequences
    sums = sums[:count] + sums[count : 2 * count] + sums[2 * count :]
    running = jnp.zeros((sequences, LANES), F32)
    suffixes = [None] * tiles
    for t in reversed(range(tiles)):
        block = sums[t * sequences : (t + 1) * sequences]
        suffixes[t] = block[:, :LANES] + running
        running = running + block[:, LANES:]
    suffix = jnp.concatenate(suffixes, axis=1)
    weights = jnp.where(usable, jnp.exp(log_gate + suffix), 0.0).astype(BF16)
    values = jnp.concatenate([values_ref[b] for b in range(sequences)], axis=1)
    products = jnp.dot(weights, values, preferred_element_type=F32)
    out = jnp.zeros((sequences, head_size), F32)
    for b in range(sequences):
        out = jnp.where(row == b, products[:, b * head_size : (b + 1) * head_size], out)
    lane = lax.broadcasted_iota(jnp.int32, (2, LANES), 1)
    group = LANES // quarters
    total = jnp.zeros((2, LANES), F32)
    for c in range(quarters):
        total = jnp.where(lane // group == c, running[2 * c : 2 * c + 2], total)
    high = total.astype(BF16).astype(F32)
    total = jnp.where(lane % group < group // 2, high, total - high)
    packed = [out[2 * c : 2 * c + 2] for c in range(quarters)] + [total]
    packed = jnp.concatenate(packed, axis=1).astype(BF16)
    for device in range(packed_ref.shape[0]):
        packed_ref[device] = packed


def output_kernel(kv_order, every_ref, own_ref, partner_ref, pair_ref):
    sequences, columns = pair_ref.shape
    parity = lax.axis_index("tp") % 2
    size = len(kv_order)
    quarters = sequences // 2
    group = LANES // quarters
    parts = []
    for block_ref, offset in ((own_ref, 1 - parity), (partner_ref, parity)):
        blocks = [
            every_ref[2 * kv_order.index(n) + offset].astype(F32) for n in range(size)
        ]
        halves = jnp.concatenate([block[:, quarters * LANES :] for block in blocks], axis=0)
        totals = halves + pltpu.roll(halves, LANES - group // 2, 1)
        later_sum = jnp.zeros((2, LANES), F32)
        later_sums = [None] * size
        for n in reversed(range(size)):
            later_sums[n] = later_sum
            later_sum = later_sum + totals[2 * n : 2 * n + 2]
        factors = jnp.exp(jnp.concatenate(later_sums, axis=0))
        rows = []
        for c in range(quarters):
            attended = jnp.zeros((2, LANES), F32)
            for n in reversed(range(size)):
                factor = factors[2 * n : 2 * n + 2, c * group : c * group + 1]
                attended = attended + blocks[n][:, c * LANES : (c + 1) * LANES] * factor
            rows.append(attended)
        attended = jnp.concatenate(rows, axis=0)
        mean_sq = jnp.mean(attended * attended, axis=1, keepdims=True)
        gain = block_ref[LANES : LANES + 16, :LANES].astype(F32)
        gain = gain[0:1] + gain[1:2] + gain[2:3]
        normed = (attended * lax.rsqrt(mean_sq + EPS) * gain).astype(BF16)
        part = jnp.dot(normed, block_ref[:LANES, :columns], preferred_element_type=F32)
        parts.append(part.astype(BF16).astype(F32))
    pair_ref[...] = parts[0] + parts[1]


def mix_kernel(*refs):
    parts = [ref[...] for ref in refs[:-1]]
    while len(parts) > 1:
        parts = [parts[i] + parts[i + 1] for i in range(0, len(parts), 2)]
    refs[-1][...] = parts[0].astype(BF16)


def led_by(leader, size):
    return [leader] + [i for i in range(size) if i != leader]


def shards(
    tokens, in_gain, w_query, score_bias, cache_keys, cache_values, lengths, head_gain, w_out
):
    sequences, features = tokens.shape
    head_width = cache_keys.shape[2]
    assert score_bias.shape[0] == 1 and head_width == LANES
    kv_size = lax.axis_size("kv")
    tp_size = lax.axis_size("tp")
    columns = w_out.shape[1]
    pairs = tp_size // 2
    assert tp_size % 2 == 0 and pairs & (pairs - 1) == 0
    seed = pl.pallas_call(
        opening_kernel,
        out_shape=pltpu.VMEM((sequences, LANES), F32),
        out_specs=VMEM,
        compiler_params=pltpu.CompilerParams(vmem_limit_bytes=1 << 20),
        cost_estimate=pl.CostEstimate(flops=1 << 33, bytes_accessed=128 << 20, transcendentals=0),
    )()
    packed, side, block = pl.pallas_call(
        query_kernel,
        out_shape=(
            jax.ShapeDtypeStruct((2 * kv_size, 2, (sequences // 2 + 1) * LANES), F32),
            jax.ShapeDtypeStruct((2 * sequences, LANES), F32),
            jax.ShapeDtypeStruct((head_width + 16, max(columns, LANES)), BF16),
        ),
        in_specs=[VMEM] * 8,
        out_specs=(VMEM,) * 3,
        compiler_params=pltpu.CompilerParams(vmem_limit_bytes=4 << 20),
        cost_estimate=pl.CostEstimate(
            flops=1 << 20, bytes_accessed=1 << 16, transcendentals=0
        ),
    )(seed, tokens, in_gain[None], w_query, score_bias[None], lengths[None], head_gain[None], w_out)
    partner = lax.ppermute(block, "tp", [(i, i ^ 1) for i in range(tp_size)])
    first = led_by(kv_size * 5 // 8, kv_size)
    groups = [
        [n * tp_size + 2 * pair + parity for n in first for parity in (1, 0)]
        for pair in range(pairs)
    ]
    gathered = lax.all_to_all(
        packed, ("kv", "tp"), 0, 0, axis_index_groups=groups, tiled=False
    )
    packed = pl.pallas_call(
        functools.partial(attention_kernel, features * kv_size),
        out_shape=jax.ShapeDtypeStruct((2 * kv_size, 2, (sequences // 2 + 1) * LANES), BF16),
        in_specs=[VMEM, VMEM, VMEM, VMEM],
        out_specs=VMEM,
        compiler_params=pltpu.CompilerParams(vmem_limit_bytes=24 << 20),
    )(gathered, side, cache_keys, cache_values)
    packed, partner = lax.optimization_barrier((packed, partner))
    groups = [
        [n * tp_size + 2 * pair + parity for n in first for parity in (1, 0)]
        for pair in range(pairs)
    ]
    every = lax.all_to_all(
        packed, ("kv", "tp"), 0, 0, axis_index_groups=groups, tiled=False
    )
    pair_sum = pl.pallas_call(
        functools.partial(output_kernel, first),
        out_shape=jax.ShapeDtypeStruct((sequences, columns), F32),
        in_specs=[VMEM] * 3,
        out_specs=VMEM,
        compiler_params=pltpu.CompilerParams(vmem_limit_bytes=4 << 20),
    )(every, block, partner)
    sums = [pair_sum]
    for shift in range(1, pairs):
        moves = [(i, i ^ (2 * shift + 1)) for i in range(tp_size)]
        sums.append(lax.ppermute(pair_sum, "tp", moves))
    return pl.pallas_call(
        mix_kernel,
        out_shape=jax.ShapeDtypeStruct((sequences, columns), BF16),
        in_specs=[VMEM] * pairs,
        out_specs=VMEM,
        compiler_params=pltpu.CompilerParams(vmem_limit_bytes=4 << 20),
    )(*sums)


def solution(mesh):
    return jax.shard_map(
        shards,
        mesh=mesh,
        in_specs=(
            P(None, "kv"),
            P("kv"),
            P("kv", "tp"),
            P("tp"),
            P(None, "kv", "tp"),
            P(None, "kv", "tp"),
            P(),
            P("tp"),
            P("tp", "kv"),
        ),
        out_specs=P(None, "kv"),
        check_vma=False,
    )
```

```python
import functools

import jax
import jax.numpy as jnp
from jax import lax
from jax.experimental import pallas as pl
from jax.experimental.pallas import tpu as pltpu
from jax.sharding import PartitionSpec as P


EPS = 1e-06
LANES = 128
VMEM = pl.BlockSpec(memory_space=pltpu.VMEM)
SMEM = pl.BlockSpec(memory_space=pltpu.SMEM)
HBM = pl.BlockSpec(memory_space=pltpu.HBM)
F32 = jnp.float32
BF16 = jnp.bfloat16


def three_terms(value):
    high = value.astype(BF16)
    rest = value - high.astype(F32)
    middle = rest.astype(BF16)
    low = (rest - middle.astype(F32)).astype(BF16)
    return high, middle, low


def opening_kernel(seed_ref):
    seed_ref[...] = jnp.zeros_like(seed_ref)


def query_kernel(
    seed_ref, tokens_ref, in_gain_ref, w_ref, bias_ref, head_gain_ref, w_out_ref,
    packed_ref, side_ref, block_ref,
):
    side_ref[...] = bias_ref[...] + seed_ref[...]
    rows, columns = w_out_ref.shape
    if columns < block_ref.shape[1]:
        block_ref[...] = jnp.zeros_like(block_ref)
    block_ref[:rows, :columns] = w_out_ref[...]
    high, middle, low = three_terms(head_gain_ref[...])
    line = lax.broadcasted_iota(jnp.int32, (16, rows), 0)
    gains = jnp.where(line == 0, high.astype(F32), 0.0)
    gains = jnp.where(line == 1, middle.astype(F32), gains)
    gains = jnp.where(line == 2, low.astype(F32), gains)
    block_ref[rows : rows + 16, :rows] = gains.astype(BF16)
    as_float = tokens_ref[...].astype(F32)
    sequences = as_float.shape[0]
    gained = (as_float * in_gain_ref[...]).astype(BF16)
    squares = jnp.sum(as_float * as_float, axis=1, keepdims=True)
    partial_value = jnp.dot(gained, w_ref[...], preferred_element_type=F32)
    quarters = sequences // 2
    lane = lax.broadcasted_iota(jnp.int32, (2, LANES), 1)
    spread = jnp.zeros((2, LANES), F32)
    for c in range(quarters):
        spread = jnp.where(lane == c, squares[2 * c : 2 * c + 2], spread)
    packed = [partial_value[2 * c : 2 * c + 2] for c in range(quarters)] + [spread]
    packed = jnp.concatenate(packed, axis=1)
    for device in range(packed_ref.shape[0]):
        packed_ref[device] = packed


def attention_kernel(width, gathered_ref, bias_ref, lengths_ref, keys_ref, values_ref, packed_ref):
    sequences, local_len, head_size = keys_ref.shape
    parity = lax.axis_index("tp") % 2
    gathered = gathered_ref[1 - parity]
    for k in range(1, gathered_ref.shape[0] // 2):
        gathered = gathered + gathered_ref[2 * k + 1 - parity]
    quarters = sequences // 2
    row_scale = lax.rsqrt(gathered[:, quarters * head_size :] / width + EPS)
    queries = jnp.concatenate(
        [
            gathered[:, c * head_size : (c + 1) * head_size] * row_scale[:, c : c + 1]
            for c in range(quarters)
        ],
        axis=0,
    )
    row = lax.broadcasted_iota(jnp.int32, (sequences, head_size), 0)
    lane = lax.broadcasted_iota(jnp.int32, (sequences, LANES), 1)
    spread = jnp.concatenate(
        [jnp.where(row == b, queries, 0.0) for b in range(sequences)], axis=1
    ).astype(BF16)
    span = local_len // 1
    tiles = span // LANES
    bias = jnp.concatenate([bias_ref[...]] * tiles, axis=1)
    own = lax.broadcasted_iota(jnp.int32, (sequences, sequences), 0)
    own = own == lax.broadcasted_iota(jnp.int32, (sequences, sequences), 1)
    lengths = jnp.where(own, lengths_ref[...].astype(F32), 0.0)
    lengths = jnp.sum(lengths, axis=1, keepdims=True)
    here = lax.axis_index("kv") * local_len
    limit = lengths.astype(jnp.int32) - here
    r = lax.broadcasted_iota(jnp.int32, (LANES, 2 * LANES), 0)
    s = lax.broadcasted_iota(jnp.int32, (LANES, 2 * LANES), 1)
    later = jnp.where((r > s) | (s >= LANES), 1.0, 0.0).astype(BF16)
    pieces = list(reversed(range(1)))
    every_score = {}
    for p in pieces:
        keys = jnp.concatenate(
            [keys_ref[b, p * span : (p + 1) * span, :] for b in range(sequences)], axis=1
        )
        every_score[p] = lax.dot_general(
            spread, keys, (((1,), (1,)), ((), ())), preferred_element_type=F32
        )
    running = jnp.zeros((sequences, LANES), F32)
    products = jnp.zeros((sequences, sequences * head_size), F32)
    for p in pieces:
        scores = every_score[p] * head_size ** (-0.5) + bias
        usable = jnp.concatenate(
            [lane + (p * tiles + t) * LANES < limit for t in range(tiles)], axis=1
        )
        soft = jnp.log1p(jnp.exp(-jnp.abs(scores)))
        log_keep = jnp.where(usable, -jnp.maximum(scores, 0.0) - soft, 0.0)
        log_gate = jnp.minimum(scores, 0.0) - soft
        stacked = jnp.concatenate(
            [log_keep[:, t * LANES : (t + 1) * LANES] for t in range(tiles)], axis=0
        )
        terms = jnp.concatenate(three_terms(stacked), axis=0)
        sums = jnp.dot(terms, later, preferred_element_type=F32)
        count = tiles * sequences
        sums = sums[:count] + sums[count : 2 * count] + sums[2 * count :]
        suffixes = [None] * tiles
        for t in reversed(range(tiles)):
            block = sums[t * sequences : (t + 1) * sequences]
            suffixes[t] = block[:, :LANES] + running
            running = running + block[:, LANES:]
        suffix = jnp.concatenate(suffixes, axis=1)
        weights = jnp.where(usable, jnp.exp(log_gate + suffix), 0.0).astype(BF16)
        values = jnp.concatenate(
            [values_ref[b, p * span : (p + 1) * span, :] for b in range(sequences)], axis=1
        )
        products = products + jnp.dot(weights, values, preferred_element_type=F32)
    out = jnp.zeros((sequences, head_size), F32)
    for b in range(sequences):
        out = jnp.where(row == b, products[:, b * head_size : (b + 1) * head_size], out)
    high = running.astype(BF16).astype(F32)
    extra = jnp.where(lane < LANES // 2, high, running - high)
    packed = jnp.concatenate([out, extra], axis=0).astype(BF16)
    for device in range(packed_ref.shape[0]):
        packed_ref[device] = packed


def output_kernel(kv_order, every_ref, own_ref, partner_ref, pair_ref):
    sequences, columns = pair_ref.shape
    parity = lax.axis_index("tp") % 2
    size = len(kv_order)
    parts = []
    for block_ref, offset in ((own_ref, 1 - parity), (partner_ref, parity)):
        later_sum = jnp.zeros((sequences, LANES), F32)
        attended = jnp.zeros((sequences, LANES), F32)
        for n in reversed(range(size)):
            packed = every_ref[2 * kv_order.index(n) + offset].astype(F32)
            halves = packed[sequences:]
            attended = attended + packed[:sequences] * jnp.exp(later_sum)
            later_sum = later_sum + (halves + pltpu.roll(halves, LANES // 2, 1))
        mean_sq = jnp.mean(attended * attended, axis=1, keepdims=True)
        gain = block_ref[LANES : LANES + 16, :LANES].astype(F32)
        gain = gain[0:1] + gain[1:2] + gain[2:3]
        normed = (attended * lax.rsqrt(mean_sq + EPS) * gain).astype(BF16)
        part = jnp.dot(normed, block_ref[:LANES, :columns], preferred_element_type=F32)
        parts.append(part.astype(BF16).astype(F32))
    pair_ref[...] = parts[0] + parts[1]


def mix_kernel(*refs):
    parts = [ref[...] for ref in refs[:-1]]
    while len(parts) > 1:
        parts = [parts[i] + parts[i + 1] for i in range(0, len(parts), 2)]
    refs[-1][...] = parts[0].astype(BF16)


def led_by(leader, size):
    return [leader] + [i for i in range(size) if i != leader]


def shards(
    tokens, in_gain, w_query, score_bias, cache_keys, cache_values, lengths, head_gain, w_out
):
    sequences, features = tokens.shape
    head_width = cache_keys.shape[2]
    assert score_bias.shape[0] == 1 and head_width == LANES
    kv_size = lax.axis_size("kv")
    tp_size = lax.axis_size("tp")
    columns = w_out.shape[1]
    pairs = tp_size // 2
    assert tp_size % 2 == 0 and pairs & (pairs - 1) == 0
    seed = pl.pallas_call(
        opening_kernel,
        out_shape=pltpu.VMEM((sequences, LANES), F32),
        out_specs=VMEM,
        compiler_params=pltpu.CompilerParams(vmem_limit_bytes=1 << 20),
        cost_estimate=pl.CostEstimate(flops=1 << 33, bytes_accessed=128 << 20, transcendentals=0),
    )()
    packed, side, block = pl.pallas_call(
        query_kernel,
        out_shape=(
            jax.ShapeDtypeStruct((2 * kv_size, 2, (sequences // 2 + 1) * LANES), F32),
            jax.ShapeDtypeStruct((sequences, LANES), F32),
            jax.ShapeDtypeStruct((head_width + 16, max(columns, LANES)), BF16),
        ),
        in_specs=[VMEM] * 7,
        out_specs=(VMEM,) * 3,
        compiler_params=pltpu.CompilerParams(vmem_limit_bytes=4 << 20),
        cost_estimate=pl.CostEstimate(
            flops=1 << 20, bytes_accessed=1 << 16, transcendentals=0
        ),
    )(seed, tokens, in_gain[None], w_query, score_bias[None], head_gain[None], w_out)
    partner = lax.ppermute(block, "tp", [(i, i ^ 1) for i in range(tp_size)])
    first = led_by(kv_size * 5 // 8, kv_size)
    groups = [
        [n * tp_size + 2 * pair + parity for n in first for parity in (1, 0)]
        for pair in range(pairs)
    ]
    gathered = lax.all_to_all(
        packed, ("kv", "tp"), 0, 0, axis_index_groups=groups, tiled=False
    )
    packed = pl.pallas_call(
        functools.partial(attention_kernel, features * kv_size),
        out_shape=jax.ShapeDtypeStruct((2 * kv_size, 2 * sequences, LANES), BF16),
        in_specs=[VMEM] * 5,
        out_specs=VMEM,
        compiler_params=pltpu.CompilerParams(vmem_limit_bytes=24 << 20),
    )(gathered, side, lengths[None], cache_keys, cache_values)
    packed, partner = lax.optimization_barrier((packed, partner))
    groups = [
        [n * tp_size + 2 * pair + parity for n in first for parity in (1, 0)]
        for pair in range(pairs)
    ]
    every = lax.all_to_all(
        packed, ("kv", "tp"), 0, 0, axis_index_groups=groups, tiled=False
    )
    pair_sum = pl.pallas_call(
        functools.partial(output_kernel, first),
        out_shape=jax.ShapeDtypeStruct((sequences, columns), F32),
        in_specs=[VMEM] * 3,
        out_specs=VMEM,
        compiler_params=pltpu.CompilerParams(vmem_limit_bytes=4 << 20),
    )(every, block, partner)
    sums = [pair_sum]
    for shift in range(1, pairs):
        moves = [(i, i ^ (2 * shift + 1)) for i in range(tp_size)]
        sums.append(lax.ppermute(pair_sum, "tp", moves))
    return pl.pallas_call(
        mix_kernel,
        out_shape=jax.ShapeDtypeStruct((sequences, columns), BF16),
        in_specs=[VMEM] * pairs,
        out_specs=VMEM,
        compiler_params=pltpu.CompilerParams(vmem_limit_bytes=4 << 20),
    )(*sums)


def solution(mesh):
    return jax.shard_map(
        shards,
        mesh=mesh,
        in_specs=(
            P(None, "kv"),
            P("kv"),
            P("kv", "tp"),
            P("tp"),
            P(None, "kv", "tp"),
            P(None, "kv", "tp"),
            P(),
            P("tp"),
            P("tp", "kv"),
        ),
        out_specs=P(None, "kv"),
        check_vma=False,
    )
```
